128 devices in a mesh: sp: 16 (over z, x), fs: 4 (over y), tp: 2 (over core).
Axes of the slice: x: 4, y: 4, z: 4, core: 2. Of those that a mesh axis runs over, the one named last changes fastest.
Arguments:
- inputs: bfloat16 [65536, 2048], P(('fs', 'sp'), 'tp'), parts along dimension 0, may hold values from -270 to 270
- mix_gain: float32 [2048], replicated, may hold values from 0.1 to 1.9
- w_query: bfloat16 [2048, 1024], P(None, 'tp'), may hold values from -0.125 to 0.125
- w_key: bfloat16 [2048, 256], P(None, 'tp'), may hold values from -0.125 to 0.125
- w_value: bfloat16 [2048, 256], P(None, 'tp'), may hold values from -0.125 to 0.125
- query_gain: float32 [64], replicated, may hold values from 0 to 14, as said below
- key_gain: float32 [64], replicated, may hold values from 0 to 14, as said below
- sink_logit: float32 [16], P('tp'), may hold values from 3 to 7
- w_inner: bfloat16 [2048, 1024], P(None, 'tp'), may hold values from -0.125 to 0.125
- w_bmat: bfloat16 [2048, 512], P(None, 'tp'), may hold values from -0.125 to 0.125
- w_cmat: bfloat16 [2048, 512], P(None, 'tp'), may hold values from -0.125 to 0.125
- w_gate: bfloat16 [2048, 1024], P(None, 'tp'), may hold values from -0.125 to 0.125
- w_step: bfloat16 [2048, 2, 16], P(None, None, 'tp'), may hold values from -0.125 to 0.125
- conv_inner: bfloat16 [5, 1024], P(None, 'tp'), may hold values from -2.5 to 2.5
- conv_bmat: bfloat16 [5, 512], P(None, 'tp'), may hold values from -2.5 to 2.5
- conv_cmat: bfloat16 [5, 512], P(None, 'tp'), may hold values from -2.5 to 2.5
- step_bias: float32 [2, 16], P(None, 'tp'), may hold values from -1 to 1
- decay_rate: float32 [2, 16], P(None, 'tp'), may hold values from 0 to 1, as said below
- decay_offset: float32 [16384, 2, 16], P('sp', None, 'tp'), may hold values from -3 to 0, as said below
- start_state: float32 [8, 16, 64, 128], P('fs', 'tp'), parts along dimension 0, may hold values from -192 to 192
- group_gain: float32 [1024], P('tp'), may hold values from 0.1 to 1.9
- w_out_attn: bfloat16 [1024, 2048], P('tp'), may hold values from -1.5 to 1.5
- w_out_state: bfloat16 [1024, 2048], P('tp'), may hold values from -0.1875 to 0.1875
Outputs:
- mixed: bfloat16 [65536, 2048], P(('fs', 'sp', 'tp')), parts along dimension 0
The draws below stay inside these ranges and needn't reach their ends.
There are 4 independent parts, one for each index of `fs`. The reference program is written for one: setup_inputs(seed, part) draws one part's arguments, and reference() takes and returns one part's arrays. A program takes and returns all parts, laid end to end along the dimension named above; an argument that names none is the same for every part. Nothing has to cross between parts.
Inputs may be any that keep to these rules, and one draw needn't show every extreme that they name: `query_gain`: positive. `key_gain`: positive. `decay_rate`: positive. `decay_offset`: never positive.
All inputs are finite; a program needn't handle non-finite values.
Results may differ from the reference program's by a relative error of at most 0.035.
Values may be sent and summed in bfloat16 or wider, within the bound.
A program may use at most 128 MiB of HBM per device.

```python
import math
import jax
import jax.numpy as jnp
from jax import lax

D = 2048
HEAD = 64
A_HEADS = 16
A_KV = 4
MIXER_HEADS = 16
S_GROUPS = 4
STATE = 128
CONV = 5
WINDOW = 128
STATE_BLOCK = 128
TOK_DEV = 1024
SEQUENCE_LENGTH = 16384
S_INNER = 1024
N_TP = 2


def draw_inputs(key, part):
    base_key = jax.random.fold_in(key, 11)
    noise_key, row_key, column_key = jax.random.split(base_key, 3)
    row_scale = jnp.exp(jax.random.uniform(row_key, (SEQUENCE_LENGTH, 1), jnp.float32, 0.0, math.log(10.0)))
    column_ramp = jnp.exp(math.log(4.0) * jnp.arange(D, dtype=jnp.float32) / D)
    column_scale = column_ramp[None, :] * jnp.exp(jax.random.uniform(column_key, (1, D), jnp.float32, -0.5, 0.5))
    values = jnp.clip(jax.random.normal(noise_key, (SEQUENCE_LENGTH, D), jnp.float32), -4.0, 4.0)
    return (values * row_scale * column_scale).astype(jnp.bfloat16)


def gain_table(key, salt):
    gain_key = jax.random.fold_in(key, salt)
    return jax.random.uniform(gain_key, (HEAD,), jnp.float32, 0.5, 1.5)


def draw_query_gain(key, part):
    return gain_table(key, 21)


def draw_key_gain(key, part):
    return gain_table(key, 22)


def slow_heads(key):
    ranking = jax.random.permutation(jax.random.fold_in(key, 31), 2 * MIXER_HEADS)
    kept_count = MIXER_HEADS
    return (ranking < kept_count).reshape(2, MIXER_HEADS)


def base_rates(key):
    slowly = slow_heads(key)
    quick_rates = jax.random.uniform(jax.random.fold_in(key, 41), (2, MIXER_HEADS), jnp.float32, 1.5, 2.5) / STATE_BLOCK
    return jnp.where(slowly, 0.2 / SEQUENCE_LENGTH, quick_rates)


def draw_decay_rate(key, part):
    return base_rates(key)


def draw_decay_offset(key, part):
    rates = base_rates(key)
    device_blocks = SEQUENCE_LENGTH // TOK_DEV
    factor_key, position_random_key, level_random_key = jax.random.split(jax.random.fold_in(key, 51), 3)
    factors = jnp.exp(jax.random.uniform(factor_key, (device_blocks, 1, 2, MIXER_HEADS), jnp.float32, math.log(0.5), math.log(2.5)))
    constant_level = -jnp.broadcast_to(factors * rates, (device_blocks, TOK_DEV, 2, MIXER_HEADS)).reshape(SEQUENCE_LENGTH, 2, MIXER_HEADS)
    spike_position = jax.random.randint(position_random_key, (2, 2, MIXER_HEADS), 0, SEQUENCE_LENGTH)
    spike_level = jnp.log(jax.random.uniform(level_random_key, (2, 2, MIXER_HEADS), jnp.float32, 0.5, 0.8))
    spike_mask = jnp.arange(SEQUENCE_LENGTH)[:, None, None, None] == spike_position[None]
    spike_count = jnp.sum(jnp.where(spike_mask, spike_level[None], 0.0), axis=1)
    return constant_level + spike_count


def levels(key, extent, cuts, least, high):
    loudness, own = 1.0, jax.random.fold_in(key, 6)
    for dim, shards_of in cuts:
        draws = jnp.exp(jax.random.uniform(jax.random.fold_in(own, dim), (shards_of,), jnp.float32, least / len(cuts), high / len(cuts)))
        loudness = loudness * jnp.repeat(draws, extent[dim] // shards_of).reshape([-1 if axis == dim else 1 for axis in range(len(extent))])
    return loudness


def bell_draw(stream_key, extent, scale, reach, cuts=(), kind=jnp.bfloat16):
    result = jax.random.normal(stream_key, extent, jnp.float32) * scale
    if len(cuts) > 0:
        result = levels(stream_key, extent, cuts, -0.22, 0.18) * result
    return jnp.clip(result, min=-reach, max=reach).astype(kind)


def setup_inputs(seed: int = 0, part: int = 0) -> dict:
    splits = jax.random.split(jax.random.key(seed), 24)
    own_keys = jax.random.split(jax.random.fold_in(splits[23], part), 24)
    inputs = draw_inputs(jax.random.fold_in(jax.random.fold_in(splits[23], part), 71), part)
    mix_gain = jnp.clip(1.0 + 0.18 * jax.random.normal(splits[1], (D,), jnp.float32), 0.1, 1.9)
    w_query = bell_draw(splits[2], (D, A_HEADS * HEAD), D ** -0.5, 0.125, ((1, 2),))
    w_key = bell_draw(splits[3], (D, A_KV * HEAD), D ** -0.5, 0.125, ((1, 2),))
    w_value = bell_draw(splits[4], (D, A_KV * HEAD), D ** -0.5, 0.125, ((1, 2),))
    query_gain = draw_query_gain(jax.random.fold_in(splits[23], 71), part)
    key_gain = draw_key_gain(jax.random.fold_in(splits[23], 71), part)
    sink_logit = jnp.clip(3.0 + 4.0 * jax.random.uniform(splits[7], (A_HEADS,), jnp.float32) ** levels(splits[7], (A_HEADS,), ((0, 2),), -0.2, 0.2), 3.0, 7.0)
    w_inner = bell_draw(splits[8], (D, S_INNER), D ** -0.5, 0.125, ((1, 2),))
    w_bmat = bell_draw(splits[9], (D, S_GROUPS * STATE), D ** -0.5, 0.125, ((1, 2),))
    w_cmat = bell_draw(splits[10], (D, S_GROUPS * STATE), D ** -0.5, 0.125, ((1, 2),))
    w_gate = bell_draw(splits[11], (D, S_INNER), D ** -0.5, 0.125, ((1, 2),))
    w_step = bell_draw(splits[12], (D, 2, MIXER_HEADS), D ** -0.5, 0.125, ((2, 2),))
    conv_inner = bell_draw(splits[13], (CONV, S_INNER), CONV ** -0.5, 2.5, ((1, 2),))
    conv_bmat = bell_draw(splits[14], (CONV, S_GROUPS * STATE), CONV ** -0.5, 2.5, ((1, 2),))
    conv_cmat = bell_draw(splits[15], (CONV, S_GROUPS * STATE), CONV ** -0.5, 2.5, ((1, 2),))
    step_bias = jnp.clip(jax.random.uniform(splits[16], (2, MIXER_HEADS), jnp.float32, -1.0, 1.0) * levels(splits[16], (2, MIXER_HEADS), ((1, 2),), -0.4, 0.0), -1.0, 1.0)
    decay_rate = draw_decay_rate(jax.random.fold_in(splits[23], 71), part)
    decay_offset = draw_decay_offset(jax.random.fold_in(splits[23], 71), part)
    start_state = bell_draw(own_keys[19], (2, MIXER_HEADS, HEAD, STATE), (SEQUENCE_LENGTH ** 0.5 // 4), 192.0, ((1, 2),), jnp.float32)
    group_gain = jnp.clip(1.0 + 0.18 * jax.random.normal(splits[20], (S_INNER,), jnp.float32), 0.1, 1.9)
    w_out_attn = bell_draw(splits[21], (A_HEADS * HEAD, D), (A_HEADS * HEAD // 64) ** -0.5, 1.5, ((0, 2),))
    w_out_state = bell_draw(splits[22], (S_INNER, D), S_INNER ** -0.5, 0.1875, ((0, 2),))
    return dict(inputs=inputs, mix_gain=mix_gain, w_query=w_query, w_key=w_key, w_value=w_value, query_gain=query_gain, key_gain=key_gain, sink_logit=sink_logit, w_inner=w_inner, w_bmat=w_bmat, w_cmat=w_cmat, w_gate=w_gate, w_step=w_step, conv_inner=conv_inner, conv_bmat=conv_bmat, conv_cmat=conv_cmat, step_bias=step_bias, decay_rate=decay_rate, decay_offset=decay_offset, start_state=start_state, group_gain=group_gain, w_out_attn=w_out_attn, w_out_state=w_out_state)


epsilon = 1e-06
rotary_base = 10000.0

def head_norm(values, gain):
    return values * lax.rsqrt(lax.optimization_barrier(jnp.mean(values * values, axis=-1, keepdims=True)) + epsilon) * gain

def rotate(values, positions):
    half_dim = values.shape[-1] // 2
    frequency = rotary_base ** (-jnp.arange(half_dim, dtype=jnp.float32) / half_dim)
    angles = positions.astype(jnp.float32)[:, None] * frequency[None, :]
    shaped = (angles.shape[0],) + (1,) * (values.ndim - 2) + (half_dim,)
    cosine = jnp.cos(angles).reshape(shaped)
    sine_table = jnp.sin(angles).reshape(shaped)
    first_half = values[..., :half_dim]
    second_half = values[..., half_dim:]
    return jnp.concatenate([first_half * cosine - second_half * sine_table, second_half * cosine + first_half * sine_table], axis=-1)

def attend_block(queries, keys, values, sink_logit, key_pos, length):
    scores = jnp.einsum('qhgd,khd->hgqk', queries.astype(jnp.float32), keys.astype(jnp.float32)) * HEAD ** (-0.5)
    offsets = jnp.arange(3 * WINDOW) - WINDOW
    nearby = jnp.abs(offsets[None, :] - jnp.arange(WINDOW)[:, None]) <= WINDOW
    inside = (key_pos >= 0) & (key_pos < length)
    allowed = nearby & inside[None, :]
    masked = jnp.where(allowed, scores, -jnp.inf)
    highest = jnp.maximum(lax.optimization_barrier(jnp.max(masked, axis=-1, keepdims=True)), sink_logit[:, :, None, None])
    raised = jnp.exp(masked - highest)
    denominator = jnp.exp(sink_logit[:, :, None, None] - highest) + lax.optimization_barrier(jnp.sum(raised, axis=-1, keepdims=True))
    weights = (raised / denominator).astype(jnp.bfloat16)
    return jnp.einsum('hgqk,khe->qhge', weights.astype(jnp.float32), values.astype(jnp.float32)).astype(jnp.bfloat16)

def ssd_blocks(inner_act, bmat_act, cmat_act, step_size, log_decay, carry_state):
    length = inner_act.shape[0]
    number_blocks = length // STATE_BLOCK

    def split_blocks(values):
        return values.reshape((number_blocks, STATE_BLOCK) + values.shape[1:])
    causal = jnp.arange(STATE_BLOCK)[:, None] >= jnp.arange(STATE_BLOCK)[None, :]

    def advance(running, block_data):
        inner_rows, bmat_rows, cmat_rows, step_rows, decay_rows = block_data
        cumulative = jnp.cumsum(decay_rows, axis=0)
        scores = jnp.einsum('lgn,sgn->lsg', cmat_rows.astype(jnp.float32), bmat_rows.astype(jnp.float32))
        spread = jnp.where(causal[:, :, None, None], cumulative[:, None] - cumulative[None, :], -jnp.inf)
        weights = (scores[:, :, :, None] * jnp.exp(spread) * step_rows[None]).astype(jnp.bfloat16)
        within = jnp.einsum('lsgr,sgrp->lgrp', weights.astype(jnp.float32), inner_rows.astype(jnp.float32))
        carried = jnp.einsum('lgn,grpn->lgrp', cmat_rows.astype(jnp.float32), running, precision=lax.Precision.HIGHEST) * jnp.exp(cumulative)[..., None]
        fading = jnp.exp(cumulative[-1:] - cumulative)
        loaded = (inner_rows.astype(jnp.float32) * (step_rows * fading)[..., None]).astype(jnp.bfloat16)
        running = jnp.exp(cumulative[-1])[..., None, None] * running + jnp.einsum('sgrp,sgn->grpn', loaded.astype(jnp.float32), bmat_rows.astype(jnp.float32))
        return (running, within + carried)
    final_state, outputs = lax.scan(advance, carry_state, tuple((split_blocks(values) for values in (inner_act, bmat_act, cmat_act, step_size, log_decay))))
    return (final_state, outputs.reshape((length,) + outputs.shape[2:]))

def reverse_rows(values):
    return values[::-1]

def reference(inputs, mix_gain, w_query, w_key, w_value, query_gain, key_gain, sink_logit, w_inner, w_bmat, w_cmat, w_gate, w_step, conv_inner, conv_bmat, conv_cmat, step_bias, decay_rate, decay_offset, start_state, group_gain, w_out_attn, w_out_state):
    length = inputs.shape[0]
    widened = inputs.astype(jnp.float32)
    row_scale = lax.rsqrt(lax.optimization_barrier(jnp.mean(widened * widened, axis=1, keepdims=True)) + epsilon)
    scaled_in = (widened * mix_gain).astype(jnp.bfloat16)

    def project(weight):
        return row_scale * jnp.dot(scaled_in, weight, preferred_element_type=jnp.float32)
    query_proj = project(w_query).astype(jnp.bfloat16)
    key_proj = project(w_key).astype(jnp.bfloat16)
    value_proj = project(w_value).astype(jnp.bfloat16)
    inner_proj = project(w_inner).astype(jnp.bfloat16)
    bmat_proj = project(w_bmat).astype(jnp.bfloat16)
    cmat_proj = project(w_cmat).astype(jnp.bfloat16)
    gate_proj = project(w_gate).astype(jnp.bfloat16)
    step_raw = project(w_step.reshape(D, 2 * MIXER_HEADS)).reshape(length, 2, MIXER_HEADS)
    positions = jnp.arange(length, dtype=jnp.int32)
    group_size = A_HEADS // A_KV
    query_rot = rotate(head_norm(query_proj.astype(jnp.float32).reshape(length, A_HEADS, HEAD), query_gain), positions).astype(jnp.bfloat16).reshape(length, A_KV, group_size, HEAD)
    key_rot = rotate(head_norm(key_proj.astype(jnp.float32).reshape(length, A_KV, HEAD), key_gain), positions).astype(jnp.bfloat16)
    value_rows = value_proj.reshape(length, A_KV, HEAD)
    padding = ((WINDOW, WINDOW), (0, 0), (0, 0))
    key_padded = jnp.pad(key_rot, padding)
    value_padded = jnp.pad(value_rows, padding)
    sink_table = sink_logit.reshape(A_KV, group_size)

    def one_block(block_index):
        block_start = (block_index * WINDOW).astype(jnp.int32)
        query_block = lax.dynamic_slice_in_dim(query_rot, block_start, WINDOW, 0)
        key_block = lax.dynamic_slice_in_dim(key_padded, block_start, 3 * WINDOW, 0)
        value_block = lax.dynamic_slice_in_dim(value_padded, block_start, 3 * WINDOW, 0)
        key_pos = block_start - WINDOW + jnp.arange(3 * WINDOW, dtype=jnp.int32)
        return attend_block(query_block, key_block, value_block, sink_table, key_pos, length)
    attended = lax.map(one_block, jnp.arange(length // WINDOW, dtype=jnp.int32))
    attention_out = attended.reshape(length, A_HEADS * HEAD)
    mixed_rows = jnp.concatenate([inner_proj, bmat_proj, cmat_proj], axis=1)
    conv_taps = jnp.concatenate([conv_inner, conv_bmat, conv_cmat], axis=1).astype(jnp.float32)
    rim_width = CONV // 2
    framed = jnp.pad(mixed_rows, ((rim_width, rim_width), (0, 0))).astype(jnp.float32)
    conv_sum = jnp.zeros(mixed_rows.shape, jnp.float32)
    for tap_index in range(CONV):
        conv_sum = conv_sum + framed[tap_index:tap_index + length] * conv_taps[tap_index]
    activated = jax.nn.silu(conv_sum).astype(jnp.bfloat16)
    repeats = MIXER_HEADS // S_GROUPS
    state_width = S_GROUPS * STATE
    inner_act = activated[:, :S_INNER].reshape(length, S_GROUPS, repeats, HEAD)
    bmat_act = activated[:, S_INNER:S_INNER + state_width].reshape(length, S_GROUPS, STATE)
    cmat_act = activated[:, S_INNER + state_width:].reshape(length, S_GROUPS, STATE)
    step_size = jax.nn.softplus(step_raw + step_bias)
    log_decay = -decay_rate * step_size + decay_offset

    def shaped(values):
        return values.reshape(length, S_GROUPS, repeats)
    begin_fwd = start_state[0].reshape(S_GROUPS, repeats, HEAD, STATE)
    begin_bwd = start_state[1].reshape(S_GROUPS, repeats, HEAD, STATE)
    unused_fwd, output_fwd = ssd_blocks(inner_act, bmat_act, cmat_act, shaped(step_size[:, 0]), shaped(log_decay[:, 0]), begin_fwd)
    unused_bwd, output_bwd = ssd_blocks(reverse_rows(inner_act), reverse_rows(bmat_act), reverse_rows(cmat_act), reverse_rows(shaped(step_size[:, 1])), reverse_rows(shaped(log_decay[:, 1])), begin_bwd)
    state_sum = output_fwd + reverse_rows(output_bwd)
    group_width = repeats * HEAD
    gate_rows = gate_proj.astype(jnp.float32).reshape(length, S_GROUPS, group_width)
    gated = state_sum.reshape(length, S_GROUPS, group_width) * jax.nn.silu(gate_rows)
    normed = gated * lax.rsqrt(lax.optimization_barrier(jnp.mean(gated * gated, axis=-1, keepdims=True)) + epsilon)
    state_out = (normed * group_gain.reshape(S_GROUPS, group_width)).astype(jnp.bfloat16).reshape(length, S_INNER)
    attn_cols = A_HEADS * HEAD // N_TP
    state_cols = S_INNER // N_TP
    summed = jnp.zeros((length, D), jnp.float32)
    for part_index in range(N_TP):
        partial_value = jnp.dot(attention_out[:, part_index * attn_cols:(part_index + 1) * attn_cols], w_out_attn[part_index * attn_cols:(part_index + 1) * attn_cols], preferred_element_type=jnp.float32)
        partial_value = partial_value + jnp.dot(state_out[:, part_index * state_cols:(part_index + 1) * state_cols], w_out_state[part_index * state_cols:(part_index + 1) * state_cols], preferred_element_type=jnp.float32)
        summed = summed + lax.optimization_barrier(partial_value.astype(jnp.bfloat16)).astype(jnp.float32)
    return summed.astype(jnp.bfloat16)
```

```python
import math

import jax
import jax.numpy as jnp
import numpy as np
from jax import lax
from jax.experimental import pallas as pl
from jax.experimental.pallas import tpu as pltpu
from jax.sharding import PartitionSpec as P

D = 2048
HALF = 1024
TOK = 1024
BLK = 128
NB = 8
EPS = 1e-06
LOG2E = math.log2(math.e)
NEG = -1e30
MESH = pl.DeviceIdType.MESH
NT = (((1,), (1,)), ((), ()))
f32 = jnp.float32
bf16 = jnp.bfloat16


def iota(shape, dim):
    return lax.broadcasted_iota(jnp.int32, shape, dim)


def mm(a, b):
    return jnp.dot(a, b, preferred_element_type=f32)


def kernel(
    nsp,
    x, gain, wq, wk, wv, wi, wb, wc, wg, wst, qgain, kgain, sink, ci, cb, cc,
    prep, start, ggain, woa, wos, tabs, rows,
    out,
    X, XS, RS, WQ, WKV, WI, WBC, WG, WO, QM, KD, VD, KVS, KVR, MX, MXR, SG, TAPS,
    COS, SIN, STP, CUM, MT, INN, BA, CA, E1X, FL, BS, SS, SR, FS, FR, ES, ER, EF, ENT,
    WN, AT, PR, SST, SPR,
    lsem, wsem, xs_s, xs_r, hs_s, hs_r, ms_s, ms_r, ss_s, ss_r, fs_s, fs_r, es_s, es_r, ps_s, ps_r,
):
    me = lax.axis_index("sp")
    t = lax.axis_index("tp")
    peer = {"tp": 1 - t}
    left = {"sp": lax.rem(me + nsp - 1, nsp)}
    right = {"sp": lax.rem(me + 1, nsp)}

    def remote(src, dst, s, r, dev):
        return pltpu.make_async_remote_copy(
            src_ref=src, dst_ref=dst, send_sem=s, recv_sem=r, device_id=dev, device_id_type=MESH
        )

    barrier = pltpu.get_barrier_semaphore()
    pl.semaphore_signal(barrier, inc=1, device_id=peer, device_id_type=MESH)
    for j in range(1, nsp):
        pl.semaphore_signal(
            barrier, inc=1, device_id={"sp": lax.rem(me + j, nsp)}, device_id_type=MESH
        )

    own = pl.multiple_of(t * HALF, HALF)
    xl = pltpu.make_async_copy(x, X.at[:, pl.ds(own, HALF)], lsem)
    xl.start()
    loads = [
        (wq, WQ), (wk, WKV.at[:, 0:128]), (wv, WKV.at[:, 128:256]), (wi, WI),
        (wb, WBC.at[:, 0:256]), (wc, WBC.at[:, 256:512]), (wg, WG),
        (woa, WO.at[0:512]), (wos, WO.at[512:1024]),
    ]
    copies = [pltpu.make_async_copy(a, b, wsem.at[i]) for i, (a, b) in enumerate(loads)]
    for c in copies:
        c.start()

    for d in range(2):
        for q in range(4):
            SST[d, :, q * 128 : (q + 1) * 128] = start[d, q * 128 : (q + 1) * 128, :].T
    TAPS[0:5, 0:512] = ci[...].astype(f32)
    TAPS[0:5, 512:768] = cb[...].astype(f32)
    TAPS[0:5, 768:1024] = cc[...].astype(f32)
    ta_c = tabs[0, pl.ds(pl.multiple_of(me * NB, NB), NB), :]
    ta_s = tabs[1, pl.ds(pl.multiple_of(me * NB, NB), NB), :]
    tb_c = rows[0]
    tb_s = rows[1]
    sign = jnp.where(lax.rem(iota((1, 128), 1), 64) < 32, -1.0, 1.0).astype(f32)
    for b in range(NB):
        ac, as_ = ta_c[b : b + 1, :], ta_s[b : b + 1, :]
        COS[b * BLK : (b + 1) * BLK, :] = ac * tb_c - as_ * tb_s
        SIN[b * BLK : (b + 1) * BLK, :] = (as_ * tb_c + ac * tb_s) * sign

    pl.semaphore_wait(barrier, nsp)

    xc = []
    for h in range(2):
        c = remote(
            x.at[h * 512 : (h + 1) * 512, :],
            X.at[h * 512 : (h + 1) * 512, pl.ds(own, HALF)],
            xs_s.at[h], xs_r.at[h], peer,
        )
        c.start()
        xc.append(c)
    xl.wait()

    lane = iota((1, 128), 1)
    lo_half = lane < 64
    first_part = lax.rem(lane, 64) < 32
    g_row, g_col = iota((128, 128), 0), iota((128, 128), 1)
    head_mean = jnp.where(g_row // 64 == g_col // 64, 1.0 / 64, 0.0).astype(bf16)
    ones_lanes = jnp.ones((128, 128), bf16)

    def normed(v, gain_row, r0):
        ms = mm((v * v).astype(bf16), head_mean)
        n = v * lax.rsqrt(ms + EPS) * gain_row
        partner = jnp.where(first_part, pltpu.roll(n, 96, 1), pltpu.roll(n, 32, 1))
        return n * COS[pl.ds(r0, 128), :] + partner * SIN[pl.ds(r0, 128), :]

    sends = []
    for h in range(2):
        xc[h].wait_recv()
        h0 = h * 512

        @pl.loop(0, 8)
        def _(i):
            r = pl.multiple_of(i * 64, 64)
            v = X[pl.ds(h0 + r, 64), :].astype(f32)
            XS[pl.ds(r, 64), :] = (v * gain[...]).astype(bf16)
            ss = jnp.sum(v * v, axis=1, keepdims=True) * (1.0 / D)
            RS[pl.ds(h0 + r, 64), :] = jnp.broadcast_to(lax.rsqrt(ss + EPS), (64, 128))

        xs = XS[...]
        rs = RS[h0 : h0 + 512, :]
        if h == 0:
            copies[1].wait()
            copies[2].wait()
        kv = mm(xs, WKV[...])
        for i in range(4):
            r0 = h0 + i * 128
            rsi = rs[i * 128 : (i + 1) * 128]
            kvi = kv[i * 128 : (i + 1) * 128]
            kp = (kvi[:, 0:128] * rsi).astype(bf16).astype(f32)
            k = normed(kp, kgain[...], r0)
            v = kvi[:, 128:256] * rsi
            vb = v.astype(bf16).astype(f32)
            kb = k.astype(bf16).astype(f32)
            kr, vr = pltpu.roll(kb, 64, 1), pltpu.roll(vb, 64, 1)
            f0 = r0 + 128
            KD[0, f0 : f0 + 128, :] = jnp.where(lo_half, kb, kr).astype(bf16)
            KD[1, f0 : f0 + 128, :] = jnp.where(lo_half, kr, kb).astype(bf16)
            VD[0, f0 : f0 + 128, 0:128] = jnp.where(lo_half, vb, vr).astype(bf16)
            VD[1, f0 : f0 + 128, 0:128] = jnp.where(lo_half, vr, vb).astype(bf16)
            VD[0, f0 : f0 + 128, 128:256] = ones_lanes
            VD[1, f0 : f0 + 128, 128:256] = ones_lanes
            if r0 == 0 or r0 == 896:
                e = 0 if r0 == 0 else 1
                KVS[e, :, 0:128] = kb.astype(bf16)
                KVS[e, :, 128:256] = vb.astype(bf16)
        if h == 0:
            copies[3].wait()
            copies[4].wait()
            copies[5].wait()
        for w, base in ((WI, 0), (WBC, 512)):
            for n in range(2):
                p = mm(xs, w[:, n * 256 : (n + 1) * 256])
                for q in range(2):
                    MX[8 + h0 : 8 + h0 + 512, base + n * 256 + q * 128 : base + n * 256 + q * 128 + 128] = (
                        (p[:, q * 128 : (q + 1) * 128] * rs).astype(bf16).astype(f32)
                    )
        e = h
        dev = left if h == 0 else right
        c = remote(KVS.at[e], KVR.at[1 - e], hs_s.at[e], hs_r.at[1 - e], dev)
        c.start()
        sends.append(c)
        mrow = 8 if h == 0 else 8 + TOK - 8
        c = remote(MX.at[mrow : mrow + 8, :], MXR.at[1 - e], ms_s.at[e], ms_r.at[1 - e], dev)
        c.start()
        sends.append(c)
        if h == 0:
            copies[0].wait()
        sp_ = mm(xs, wst[...]) * rs
        for i in range(4):
            STP[h * 4 + i] = sp_[i * 128 : (i + 1) * 128].T[0:16]
        for n in range(2):
            p = mm(xs, WQ[:, n * 256 : (n + 1) * 256])
            for q in range(2):
                tile = 2 * n + q
                for i in range(4):
                    r0 = h0 + i * 128
                    qp = (
                        (p[i * 128 : (i + 1) * 128, q * 128 : (q + 1) * 128] * rs[i * 128 : (i + 1) * 128])
                        .astype(bf16)
                        .astype(f32)
                    )
                    v = normed(qp, qgain[...], r0)
                    QM[2 * tile, r0 : r0 + 128, :] = jnp.where(lo_half, v, 0.0).astype(bf16)
                    QM[2 * tile + 1, r0 : r0 + 128, :] = jnp.where(lo_half, 0.0, v).astype(bf16)
        if h == 0:
            copies[6].wait()
        for n in range(2):
            p = mm(xs, WG[:, n * 256 : (n + 1) * 256])
            for q in range(2):
                gp = (p[:, q * 128 : (q + 1) * 128] * rs).astype(bf16).astype(f32)
                SG[h0 : h0 + 512, n * 256 + q * 128 : n * 256 + (q + 1) * 128] = gp / (1.0 + jnp.exp(-gp))

    bias = prep[:, TOK : TOK + 1]
    rate = prep[:, TOK + 128 : TOK + 129]
    lane8 = iota((8, 128), 1)
    for b in range(NB):
        v = STP[b] + bias
        step = jnp.maximum(v, 0.0) + jnp.log1p(jnp.exp(-jnp.abs(v)))
        la = -rate * step + prep[:, b * BLK : (b + 1) * BLK]
        cf, cw = la[0:8], la[8:16]
        for k in (1, 2, 4, 8, 16, 32, 64):
            cf = cf + jnp.where(lane8 >= k, pltpu.roll(cf, k, 1), 0.0)
            cw = cw + jnp.where(lane8 < 128 - k, pltpu.roll(cw, 128 - k, 1), 0.0)
        cum = jnp.concatenate([cf, cw], axis=0)
        last = jnp.concatenate([cf[:, 127:128], cw[:, 0:1]], axis=0)
        e1 = jnp.exp(cum)
        e2 = step * jnp.exp(last - cum)
        STP[b] = step
        CUM[b] = cum
        MT[b * BLK : (b + 1) * BLK, :] = jnp.concatenate(
            [cum, e1, e2, jnp.zeros((80, 128), f32)], axis=0
        ).T

    def halo_in(e):
        remote(MX.at[8:16, :], MXR.at[e], ms_s.at[e], ms_r.at[e], left).wait_recv()

    ex_row, ex_col = lax.rem(iota((256, 1024), 0), 128), iota((256, 1024), 1) // 64
    SPR[0] = jnp.where(ex_row == ex_col + 16, 1.0, 0.0).astype(bf16)
    SPR[1] = jnp.where(ex_row == ex_col + 32, 1.0, 0.0).astype(bf16)

    def pre_block(b):
        r0 = pl.multiple_of(b * BLK, BLK)
        m = MT[pl.ds(r0, 128), :]
        hi = m.astype(bf16)
        lo = (m - hi.astype(f32)).astype(bf16)
        both = jnp.concatenate([hi, lo], axis=1)
        bts = [None, None]
        for ct in (4, 5, 6, 7, 0, 1, 2, 3):
            w = MX[pl.ds(r0, 144), ct * 128 : (ct + 1) * 128]
            acc = None
            for j in range(5):
                term = pltpu.roll(w, 144 - (6 + j), 0)[0:128] * TAPS[j : j + 1, ct * 128 : (ct + 1) * 128]
                acc = term if acc is None else acc + term
            act = (acc / (1.0 + jnp.exp(-acc))).astype(bf16)
            if ct >= 6:
                CA[pl.ds(r0, 128), (ct - 6) * 128 : (ct - 5) * 128] = act
            elif ct >= 4:
                BA[pl.ds(r0, 128), (ct - 4) * 128 : (ct - 3) * 128] = act
                bts[ct - 4] = act.astype(f32).T.astype(bf16)
            else:
                INN[pl.ds(r0, 128), ct * 128 : (ct + 1) * 128] = act
                g = ct // 2
                for d in range(2):
                    c0 = d * 512 + ct * 128
                    e2x = mm(both, SPR[1, :, c0 : c0 + 128])
                    loaded = (act.astype(f32) * e2x).astype(bf16)
                    BS[b, :, c0 : c0 + 128] = mm(bts[g], loaded)
        return both

    def pre_all(b):
        both = pre_block(b)
        r0 = pl.multiple_of(b * BLK, BLK)
        e1x = mm(both, SPR[0])
        return r0, e1x

    def pre_step(b):
        r0, e1x = pre_all(b)
        E1X[pl.ds(r0, 128), :] = e1x
        FL[b, 0:1, 0:512] = e1x[127:128, 0:512]
        FL[b, 0:1, 512:1024] = e1x[0:1, 512:1024]

    @pl.loop(1, 7)
    def _(b):
        pre_step(b)

    halo_in(0)
    halo_in(1)
    MX[0:8, :] = jnp.where(me == 0, 0.0, MXR[0])
    MX[8 + TOK : 16 + TOK, :] = jnp.where(me == nsp - 1, 0.0, MXR[1])

    @pl.loop(0, 2)
    def _(i):
        pre_step(i * 7)

    fd = FL[0, 0:1, :]
    for b in range(1, NB):
        fd = fd * FL[b, 0:1, :]
    FS[...] = jnp.concatenate([fd[:, i * 128 : (i + 1) * 128] for i in range(8)], axis=0)
    FR[me] = FS[...]

    def chain_out(k):
        n0 = pl.multiple_of(k * 8, 8)
        rf = jnp.zeros((8, 512), f32)
        rb = jnp.zeros((8, 512), f32)
        for b in range(NB):
            rf = FL[b, 0:1, 0:512] * rf + BS[b, pl.ds(n0, 8), 0:512]
            z = NB - 1 - b
            rb = FL[z, 0:1, 512:1024] * rb + BS[z, pl.ds(n0, 8), 512:1024]
        return jnp.concatenate([rf, rb], axis=0).astype(bf16)

    SR[me] = chain_out(me)

    @pl.loop(1, nsp)
    def _(j):
        k = lax.rem(me + j, nsp)
        SS[k] = chain_out(k)
        remote(FS, FR.at[me], fs_s.at[k], fs_r.at[me], {"sp": k}).start()
        remote(SS.at[k], SR.at[me], ss_s.at[k], ss_r.at[me], {"sp": k}).start()

    def kv_halo(e):
        remote(KVS.at[e], KVR.at[e], hs_s.at[e], hs_r.at[e], left).wait_recv()
        kb = KVR[e, :, 0:128].astype(f32)
        vb = KVR[e, :, 128:256].astype(f32)
        kr, vr = pltpu.roll(kb, 64, 1), pltpu.roll(vb, 64, 1)
        f0 = 0 if e == 0 else 128 + TOK
        KD[0, f0 : f0 + 128, :] = jnp.where(lo_half, kb, kr).astype(bf16)
        KD[1, f0 : f0 + 128, :] = jnp.where(lo_half, kr, kb).astype(bf16)
        VD[0, f0 : f0 + 128, 0:128] = jnp.where(lo_half, vb, vr).astype(bf16)
        VD[1, f0 : f0 + 128, 0:128] = jnp.where(lo_half, vr, vb).astype(bf16)
        VD[0, f0 : f0 + 128, 128:256] = ones_lanes
        VD[1, f0 : f0 + 128, 128:256] = ones_lanes

    kv_halo(0)
    kv_halo(1)

    def attend(b):
        r0 = pl.multiple_of(b * BLK, BLK)
        off_l = jnp.where((me == 0) & (b == 0), 1024, 0)
        off_r = jnp.where((me == nsp - 1) & (b == NB - 1), 1024, 0)
        keep_l = g_col >= g_row + off_l
        keep_r = g_col <= g_row - off_r
        for g in range(2):
            kk = KD[g, pl.ds(r0, 384), :]
            vv = VD[g, pl.ds(r0, 384), :]
            for pair in range(2):
                res = []
                for j in range(2):
                    h = g * 4 + pair * 2 + j
                    s = lax.dot_general(QM[h, pl.ds(r0, 128), :], kk, NT, preferred_element_type=f32)
                    sl = jnp.where(keep_l, s[:, 0:128], NEG)
                    sm = s[:, 128:256]
                    sr = jnp.where(keep_r, s[:, 256:384], NEG)
                    sk = sink[h] * LOG2E
                    m = jnp.max(jnp.maximum(jnp.maximum(sl, sm), sr), axis=1, keepdims=True)
                    m = jnp.broadcast_to(jnp.maximum(m, sk), (128, 128))
                    p = jnp.concatenate(
                        [jnp.exp2(v - m).astype(bf16) for v in (sl, sm, sr)], axis=1
                    )
                    o = mm(p, vv)
                    res.append(o[:, 0:128] / (o[:, 128:256] + jnp.exp2(sk - m)))
                tile = g * 2 + pair
                AT[pl.ds(r0, 128), tile * 128 : (tile + 1) * 128] = jnp.where(
                    lo_half, res[0], res[1]
                ).astype(bf16)

    def inside(b):
        r0 = pl.multiple_of(b * BLK, BLK)
        lower = g_row >= g_col
        diag = g_row == g_col
        for g in range(2):
            cm = CA[pl.ds(r0, 128), g * 128 : (g + 1) * 128]
            bm = BA[pl.ds(r0, 128), g * 128 : (g + 1) * 128]
            sc = lax.dot_general(cm, bm, NT, preferred_element_type=f32)
            for pair in range(2):
                tile = g * 2 + pair
                xt = INN[pl.ds(r0, 128), tile * 128 : (tile + 1) * 128].astype(f32)
                ws = []
                for j in range(2):
                    h = tile * 2 + j
                    dif = jnp.where(
                        lower,
                        MT[pl.ds(r0, 128), h : h + 1] - CUM[b, h : h + 1, :],
                        MT[pl.ds(r0, 128), 8 + h : 9 + h] - CUM[b, 8 + h : 9 + h, :],
                    )
                    sf, sb = STP[b, h : h + 1, :], STP[b, 8 + h : 9 + h, :]
                    st = jnp.where(diag, sf + sb, jnp.where(lower, sf, sb))
                    ws.append((sc * jnp.exp(dif) * st).astype(bf16))
                both = jnp.concatenate(ws, axis=1)
                xx = jnp.concatenate(
                    [jnp.where(lo_half, xt, 0.0).astype(bf16), jnp.where(lo_half, 0.0, xt).astype(bf16)],
                    axis=0,
                )
                WN[pl.ds(r0, 128), tile * 128 : (tile + 1) * 128] = mm(both, xx)

    @pl.loop(0, 5)
    def _(b):
        attend(b)

    for j in range(1, nsp):
        k = lax.rem(me + j, nsp)
        remote(FS, FR.at[k], fs_s.at[k], fs_r.at[k], {"sp": k}).wait_recv()
        remote(SS.at[k], SR.at[k], ss_s.at[k], ss_r.at[k], {"sp": k}).wait_recv()

    n0 = pl.multiple_of(me * 8, 8)

    def decay_row(d, which):
        return jnp.concatenate([FR[d, which * 4 + i : which * 4 + i + 1, :] for i in range(4)], axis=1)

    run = SST[0, pl.ds(n0, 8), :]
    for d in range(nsp):
        EF[d] = run
        run = decay_row(d, 0) * run + SR[d].astype(f32)[0:8]
    run = SST[1, pl.ds(n0, 8), :]
    for d in range(nsp - 1, -1, -1):
        ES[d] = jnp.concatenate([EF[d], run], axis=0).astype(bf16)
        run = decay_row(d, 1) * run + SR[d].astype(f32)[8:16]
    ER[me] = ES[me]

    @pl.loop(1, nsp)
    def _(j):
        k = lax.rem(me + j, nsp)
        remote(ES.at[k], ER.at[me], es_s.at[k], es_r.at[me], {"sp": k}).start()

    @pl.loop(5, NB)
    def _(b):
        attend(b)

    @pl.loop(0, NB)
    def _(b):
        inside(b)

    for j in range(1, nsp):
        k = lax.rem(me + j, nsp)
        remote(ES.at[k], ER.at[k], es_s.at[k], es_r.at[k], {"sp": k}).wait_recv()

    @pl.loop(0, 8)
    def _(i):
        n1 = pl.multiple_of(i * 16, 16)
        ea = ER[2 * i].astype(f32)
        eb = ER[2 * i + 1].astype(f32)
        rf = jnp.concatenate([ea[0:8], eb[0:8]], axis=0)
        rb = jnp.concatenate([ea[8:16], eb[8:16]], axis=0)
        for b in range(NB):
            ENT[b, pl.ds(n1, 16), 0:512] = rf.astype(bf16)
            rf = FL[b, 0:1, 0:512] * rf + BS[b, pl.ds(n1, 16), 0:512]
            z = NB - 1 - b
            ENT[z, pl.ds(n1, 16), 512:1024] = rb.astype(bf16)
            rb = FL[z, 0:1, 512:1024] * rb + BS[z, pl.ds(n1, 16), 512:1024]

    group_mean = jnp.full((256, 256), 1.0 / 256, bf16)

    def finish(b):
        r0 = pl.multiple_of(b * BLK, BLK)
        for g in range(2):
            cm = CA[pl.ds(r0, 128), g * 128 : (g + 1) * 128]
            c0, c1 = g * 256, (g + 1) * 256
            tot = (
                WN[pl.ds(r0, 128), c0:c1]
                + mm(cm, ENT[b, :, c0:c1]) * E1X[pl.ds(r0, 128), c0:c1]
                + mm(cm, ENT[b, :, 512 + c0 : 512 + c1]) * E1X[pl.ds(r0, 128), 512 + c0 : 512 + c1]
            )
            gated = tot * SG[pl.ds(r0, 128), c0:c1]
            ms = mm((gated * gated).astype(bf16), group_mean)
            AT[pl.ds(r0, 128), 512 + c0 : 512 + c1] = (
                gated * lax.rsqrt(ms + EPS) * ggain[0:1, c0:c1]
            ).astype(bf16)

    copies[7].wait()
    copies[8].wait()
    other = pl.multiple_of((1 - t) * 512, 512)
    mine = pl.multiple_of(t * 512, 512)
    pc = []

    @pl.loop(0, 4)
    def _(i):
        finish((1 - t) * 4 + i)

    for n in range(4):
        XS[:, n * 512 : (n + 1) * 512] = mm(
            AT[pl.ds(other, 512), :], WO[:, n * 512 : (n + 1) * 512]
        ).astype(bf16)
        c = remote(
            XS.at[:, n * 512 : (n + 1) * 512], PR.at[:, n * 512 : (n + 1) * 512],
            ps_s.at[n], ps_r.at[n], peer,
        )
        c.start()
        pc.append(c)

    @pl.loop(0, 4)
    def _(i):
        finish(t * 4 + i)

    for n in range(4):
        p = mm(AT[pl.ds(mine, 512), :], WO[:, n * 512 : (n + 1) * 512]).astype(bf16).astype(f32)
        pc[n].wait_recv()
        out[:, n * 512 : (n + 1) * 512] = (
            p + PR[:, n * 512 : (n + 1) * 512].astype(f32)
        ).astype(bf16)

    for c in xc + sends + pc:
        c.wait_send()

    @pl.loop(1, nsp)
    def _(j):
        k = lax.rem(me + j, nsp)
        remote(FS, FR.at[me], fs_s.at[k], fs_r.at[me], {"sp": k}).wait_send()
        remote(SS.at[k], SR.at[me], ss_s.at[k], ss_r.at[me], {"sp": k}).wait_send()
        remote(ES.at[k], ER.at[me], es_s.at[k], es_r.at[me], {"sp": k}).wait_send()


def tables(blocks):
    freq = 10000.0 ** (-(np.arange(128) % 32) / 32.0)
    a = np.arange(blocks)[:, None] * 128.0 * freq[None, :]
    r = np.arange(128)[:, None] * freq[None, :]
    return (
        np.stack([np.cos(a), np.sin(a)]).astype(np.float32),
        np.stack([np.cos(r), np.sin(r)]).astype(np.float32),
    )


def local(
    nsp, inputs, mix_gain, w_query, w_key, w_value, query_gain, key_gain, sink_logit, w_inner, w_bmat, w_cmat,
    w_gate, w_step, conv_inner, conv_bmat, conv_cmat, step_bias, decay_rate, decay_offset, start_state,
    group_gain, w_out_attn, w_out_state,
):
    wst = jnp.pad(w_step.reshape(D, 16), ((0, 0), (0, 112)))
    qgain = (jnp.tile(query_gain, 2) * (LOG2E / 8.0)).reshape(1, 128)
    kgain = jnp.tile(key_gain, 2).reshape(1, 128)
    off = jnp.transpose(decay_offset, (1, 2, 0)).reshape(16, TOK)
    prep = jnp.concatenate(
        [
            off,
            jnp.broadcast_to(step_bias.reshape(16, 1), (16, 128)),
            jnp.broadcast_to(decay_rate.reshape(16, 1), (16, 128)),
        ],
        axis=1,
    )
    tabs, rows = tables(nsp * NB)
    hbm = pl.BlockSpec(memory_space=pl.ANY)
    vm = pl.BlockSpec(memory_space=pltpu.VMEM)
    sm = pl.BlockSpec(memory_space=pltpu.SMEM)
    V = pltpu.VMEM
    dma = pltpu.SemaphoreType.DMA
    return pl.pallas_call(
        lambda *refs: kernel(nsp, *refs),
        name="layer",
        out_shape=jax.ShapeDtypeStruct((TOK // 2, D), bf16),
        in_specs=[hbm, vm, hbm, hbm, hbm, hbm, hbm, hbm, hbm, vm, vm, vm, sm, vm, vm, vm, vm, vm, vm, hbm, hbm, vm, vm],
        out_specs=vm,
        scratch_shapes=[
            V((TOK, D), bf16), V((512, D), bf16), V((TOK, 128), f32),
            V((D, 512), bf16), V((D, 256), bf16), V((D, 512), bf16), V((D, 512), bf16), V((D, 512), bf16),
            V((1024, D), bf16),
            V((8, TOK, 128), bf16), V((2, TOK + 256, 128), bf16), V((2, TOK + 256, 256), bf16),
            V((2, 128, 256), bf16), V((2, 128, 256), bf16),
            V((TOK + 16, 1024), f32), V((2, 8, 1024), f32), V((TOK, 512), f32), V((8, 1024), f32),
            V((TOK, 128), f32), V((TOK, 128), f32),
            V((NB, 16, 128), f32), V((NB, 16, 128), f32), V((TOK, 128), f32),
            V((TOK, 512), bf16), V((TOK, 256), bf16), V((TOK, 256), bf16),
            V((TOK, 1024), f32), V((NB, 8, 1024), f32), V((NB, 128, 1024), f32),
            V((nsp, 16, 512), bf16), V((nsp, 16, 512), bf16), V((8, 128), f32), V((nsp, 8, 128), f32),
            V((nsp, 16, 512), bf16), V((nsp, 16, 512), bf16), V((nsp, 8, 512), f32),
            V((NB, 128, 1024), bf16),
            V((TOK, 512), f32), V((TOK, 1024), bf16), V((512, D), bf16), V((2, 128, 512), f32), V((2, 256, 1024), bf16),
            dma, dma((9,)), dma((2,)), dma((2,)), dma((2,)), dma((2,)), dma((2,)), dma((2,)),
            dma((nsp,)), dma((nsp,)), dma((nsp,)), dma((nsp,)), dma((nsp,)), dma((nsp,)), dma((4,)), dma((4,)),
        ],
        compiler_params=pltpu.CompilerParams(
            collective_id=0, has_side_effects=True, vmem_limit_bytes=64 * 1024 * 1024 - 65536
        ),
    )(
        inputs, mix_gain.reshape(1, D), w_query, w_key, w_value, w_inner, w_bmat, w_cmat, w_gate, wst,
        qgain, kgain, sink_logit, conv_inner, conv_bmat, conv_cmat, prep, start_state.reshape(2, 512, 128),
        group_gain.reshape(1, 512), w_out_attn, w_out_state, jnp.asarray(tabs), jnp.asarray(rows),
    )


def solution(mesh):
    nsp = mesh.shape["sp"]
    return jax.shard_map(
        lambda *args: local(nsp, *args),
        mesh=mesh,
        in_specs=(
            P(("fs", "sp"), "tp"), P(), P(None, "tp"), P(None, "tp"), P(None, "tp"), P(), P(), P("tp"),
            P(None, "tp"), P(None, "tp"), P(None, "tp"), P(None, "tp"), P(None, None, "tp"),
            P(None, "tp"), P(None, "tp"), P(None, "tp"), P(None, "tp"), P(None, "tp"),
            P("sp", None, "tp"), P("fs", "tp", None, None), P("tp"), P("tp", None), P("tp", None),
        ),
        out_specs=P(("fs", "sp", "tp"), None),
        check_vma=False,
    )
```

```python
import math

import jax
import jax.numpy as jnp
import numpy as np
from jax import lax
from jax.experimental import pallas as pl
from jax.experimental.pallas import tpu as pltpu
from jax.sharding import PartitionSpec as P

D = 2048
HALF = 1024
TOK = 1024
BLK = 128
NB = 8
EPS = 1e-06
LOG2E = math.log2(math.e)
NEG = -1e30
MESH = pl.DeviceIdType.MESH
NT = (((1,), (1,)), ((), ()))
f32 = jnp.float32
bf16 = jnp.bfloat16


def iota(shape, dim):
    return lax.broadcasted_iota(jnp.int32, shape, dim)


def mm(a, b):
    return jnp.dot(a, b, preferred_element_type=f32)


def silu(v):
    h = 0.5 * v
    return h + h * jnp.tanh(h)


def kernel(
    nsp,
    x, gain, wq, wk, wv, wi, wb, wc, wg, wst, qgain, kgain, sink, ci, cb, cc,
    bias, rate, off, start, ggain, woa, wos, tabs, rows,
    out,
    XO0, XO1, XP0, XP1, RS, WQ, WKV, WI, WBC, WG, WO, WST, QM, KD, VD, KVS, KVR, MX, MXR, SG, TAPS,
    COS, SIN, STP, CUM, MT, INN, BA, CA, E1X, FL, BS, SS, SR, FS, FR, ES, ER, EF, ENT,
    WN, AT, PR, SST, SPR, HM, STV, TBV, RWV,
    lsem, wsem, xs_s, xs_r, hs_s, hs_r, ms_s, ms_r, ss_s, ss_r, fs_s, fs_r, es_s, es_r, ps_s, ps_r, osem,
):
    me = lax.axis_index("sp")
    t = lax.axis_index("tp")
    peer = {"tp": 1 - t}
    left = {"sp": lax.rem(me + nsp - 1, nsp)}
    right = {"sp": lax.rem(me + 1, nsp)}
    XO, XP = (XO0, XO1), (XP0, XP1)

    def remote(src, dst, s, r, dev):
        return pltpu.make_async_remote_copy(
            src_ref=src, dst_ref=dst, send_sem=s, recv_sem=r, device_id=dev, device_id_type=MESH
        )

    barrier = pltpu.get_barrier_semaphore()
    pl.semaphore_signal(barrier, inc=1, device_id=peer, device_id_type=MESH)
    for j in range(1, nsp):
        pl.semaphore_signal(
            barrier, inc=1, device_id={"sp": lax.rem(me + j, nsp)}, device_id_type=MESH
        )

    own = pl.multiple_of(t * HALF, HALF)
    oth = pl.multiple_of((1 - t) * HALF, HALF)
    xl = [pltpu.make_async_copy(x.at[h * 512 : (h + 1) * 512, :], XO[h], lsem.at[h]) for h in range(2)]
    small = [
        pltpu.make_async_copy(start, STV, lsem.at[2]),
        pltpu.make_async_copy(tabs.at[:, pl.ds(pl.multiple_of(me * NB, NB), NB), :], TBV, lsem.at[3]),
        pltpu.make_async_copy(rows, RWV, lsem.at[4]),
    ]
    pieces = [(wk, WKV, 0, 128), (wv, WKV, 128, 128), (wi, WI, 0, 512), (wb, WBC, 0, 256), (wc, WBC, 256, 256)]
    first = [
        pltpu.make_async_copy(w.at[pl.ds(own, HALF), :], d.at[pl.ds(own, HALF), c0 : c0 + n], wsem.at[i])
        for i, (w, d, c0, n) in enumerate(pieces)
    ]
    second = [
        pltpu.make_async_copy(w.at[pl.ds(oth, HALF), :], d.at[pl.ds(oth, HALF), c0 : c0 + n], wsem.at[5 + i])
        for i, (w, d, c0, n) in enumerate(pieces)
    ]
    third = [
        pltpu.make_async_copy(wq, WQ, wsem.at[10]),
        pltpu.make_async_copy(wg, WG, wsem.at[11]),
        pltpu.make_async_copy(woa, WO.at[0:512], wsem.at[12]),
        pltpu.make_async_copy(wos, WO.at[512:1024], wsem.at[13]),
    ]
    for c in [xl[0]] + first + [xl[1]] + small + second + third:
        c.start()

    lane = iota((1, 128), 1)
    lo_half = lane < 64
    first_part = lax.rem(lane, 64) < 32
    g_row, g_col = iota((128, 128), 0), iota((128, 128), 1)
    ones_lanes = jnp.ones((128, 128), bf16)
    HM[...] = jnp.where(iota((256, 256), 0) // 64 == iota((256, 256), 1) // 64, 1.0 / 64, 0.0).astype(bf16)
    WST[...] = jnp.zeros((128, D), bf16)
    WST[0:16, :] = wst[...]
    TAPS[0:5, 0:512] = ci[...].astype(f32)
    TAPS[0:5, 512:768] = cb[...].astype(f32)
    TAPS[0:5, 768:1024] = cc[...].astype(f32)
    qg = jnp.concatenate([qgain[...], qgain[...]], axis=1) * (LOG2E / 8.0)
    kg = jnp.concatenate([kgain[...], kgain[...]], axis=1)

    def scale(ref, off_, h, begin):
        g = gain[0:1, pl.ds(off_, HALF)]
        for i in range(8):
            r = i * 64
            v = ref[r : r + 64, :].astype(f32)
            ref[r : r + 64, :] = (v * g).astype(bf16)
            ss = jnp.broadcast_to(jnp.sum(v * v, axis=1, keepdims=True), (64, 128))
            if begin:
                RS[h, r : r + 64, :] = ss
            else:
                RS[h, r : r + 64, :] = lax.rsqrt((RS[h, r : r + 64, :] + ss) * (1.0 / D) + EPS)

    mixed_tiles = [(WI, 0), (WI, 256), (WBC, 0), (WBC, 256)]

    def part_one(h):
        rows_ = slice(h * 512, (h + 1) * 512)
        xs = XO[h][...]
        WN[rows_, 0:256] = mm(xs, WKV[pl.ds(own, HALF), :])
        WN[rows_, 256:384] = lax.dot_general(xs, WST[:, pl.ds(own, HALF)], NT, preferred_element_type=f32)
        if h == 0:
            for c in first[2:]:
                c.wait()
        for n, (w, c0) in enumerate(mixed_tiles):
            E1X[rows_, n * 256 : (n + 1) * 256] = mm(xs, w[pl.ds(own, HALF), c0 : c0 + 256])

    xl[0].wait()
    scale(XO[0], own, 0, True)
    first[0].wait()
    first[1].wait()
    part_one(0)
    with jax.named_scope("w_barrier"):
        pl.semaphore_wait(barrier, nsp)
    xc = []
    for h in range(2):
        c = remote(x.at[h * 512 : (h + 1) * 512, :], XP[h], xs_s.at[h], xs_r.at[h], peer)
        c.start()
        xc.append(c)
    xl[1].wait()
    scale(XO[1], own, 1, True)
    part_one(1)

    for c in small:
        c.wait()
    for d in range(2):
        for q in range(4):
            SST[d, :, q * 128 : (q + 1) * 128] = STV[d, q * 128 : (q + 1) * 128, :].T
    sign = jnp.where(first_part, -1.0, 1.0).astype(f32)
    for b in range(NB):
        ac, as_ = TBV[0, b : b + 1, :], TBV[1, b : b + 1, :]
        COS[b * BLK : (b + 1) * BLK, :] = ac * RWV[0] - as_ * RWV[1]
        SIN[b * BLK : (b + 1) * BLK, :] = (as_ * RWV[0] + ac * RWV[1]) * sign
    for d in range(2):
        ex_row, ex_col = lax.rem(iota((256, 1024), 0), 128), iota((256, 1024), 1) // 64
        SPR[d] = jnp.where(ex_row == ex_col + 16 * (d + 1), 1.0, 0.0).astype(bf16)

    def rotated(n, r0):
        partner = jnp.where(first_part, pltpu.roll(n, 96, 1), pltpu.roll(n, 32, 1))
        return n * COS[r0 : r0 + 128, :] + partner * SIN[r0 : r0 + 128, :]

    def keep_kv(kb, vb, f0):
        kr, vr = pltpu.roll(kb, 64, 1), pltpu.roll(vb, 64, 1)
        KD[0, f0 : f0 + 128, :] = jnp.where(lo_half, kb, kr).astype(bf16)
        KD[1, f0 : f0 + 128, :] = jnp.where(lo_half, kr, kb).astype(bf16)
        VD[0, f0 : f0 + 128, 0:128] = jnp.where(lo_half, vb, vr).astype(bf16)
        VD[1, f0 : f0 + 128, 0:128] = jnp.where(lo_half, vr, vb).astype(bf16)
        VD[0, f0 : f0 + 128, 128:256] = ones_lanes
        VD[1, f0 : f0 + 128, 128:256] = ones_lanes

    sends = []

    def part_two(h):
        h0 = h * 512
        rows_ = slice(h0, h0 + 512)
        xs = XP[h][...]
        for n, (w, c0) in enumerate(mixed_tiles):
            p = mm(xs, w[pl.ds(oth, HALF), c0 : c0 + 256])
            for q in range(2):
                ct = 2 * n + q
                MX[ct, 8 + h0 : 8 + h0 + 512, :] = (
                    ((p[:, q * 128 : (q + 1) * 128] + E1X[rows_, ct * 128 : (ct + 1) * 128]) * RS[h])
                    .astype(bf16)
                    .astype(f32)
                )
        kv = mm(xs, WKV[pl.ds(oth, HALF), :])
        sp_ = lax.dot_general(xs, WST[:, pl.ds(oth, HALF)], NT, preferred_element_type=f32)
        for i in range(4):
            sub = slice(i * 128, (i + 1) * 128)
            STP[h * 4 + i] = ((sp_[sub] + WN[h0 + i * 128 : h0 + (i + 1) * 128, 256:384]) * RS[h, sub, :]).T[0:16]
        kp = ((kv[:, 0:128] + WN[rows_, 0:128]) * RS[h]).astype(bf16).astype(f32)
        vb = ((kv[:, 128:256] + WN[rows_, 128:256]) * RS[h]).astype(bf16).astype(f32)
        ms = mm((kp * kp).astype(bf16), HM[0:128, 0:128])
        for i in range(4):
            r0 = h0 + i * 128
            sub = slice(i * 128, (i + 1) * 128)
            k = rotated(kp[sub] * lax.rsqrt(ms[sub] + EPS) * kg, r0)
            kb = k.astype(bf16).astype(f32)
            keep_kv(kb, vb[sub], r0 + 128)
            if r0 == 0 or r0 == 896:
                KVS[h, :, 0:128] = kb.astype(bf16)
                KVS[h, :, 128:256] = vb[sub].astype(bf16)
        dev = left if h == 0 else right
        mrow = 8 if h == 0 else TOK
        c = remote(MX.at[:, mrow : mrow + 8, :], MXR.at[1 - h], ms_s.at[h], ms_r.at[1 - h], dev)
        c.start()
        sends.append(c)
        c = remote(KVS.at[h], KVR.at[1 - h], hs_s.at[h], hs_r.at[1 - h], dev)
        c.start()
        sends.append(c)

    for h in range(2):
        with jax.named_scope(f"w_x{h}"):
            xc[h].wait_recv()
        if h == 0:
            with jax.named_scope("w_w2"):
                for c in second:
                    c.wait()
        scale(XP[h], oth, h, False)
        part_two(h)

    with jax.named_scope("w_qg"):
        third[0].wait()
        third[1].wait()

    row16 = iota((16, 128), 0)
    bias_c = jnp.zeros((16, 128), f32)
    rate_c = jnp.zeros((16, 128), f32)
    for r in range(16):
        bias_c = jnp.where(row16 == r, bias[r // 8, r % 8], bias_c)
        rate_c = jnp.where(row16 == r, rate[r // 8, r % 8], rate_c)
    lane8 = iota((8, 128), 1)

    def steps(b):
        v = STP[b] + bias_c
        step = jnp.maximum(v, 0.0) + jnp.log1p(jnp.exp(-jnp.abs(v)))
        la = (-rate_c * step + off[:, b * BLK : (b + 1) * BLK]) * LOG2E
        cf, cw = la[0:8], la[8:16]
        for k in (1, 2, 4, 8, 16, 32, 64):
            cf = cf + jnp.where(lane8 >= k, pltpu.roll(cf, k, 1), 0.0)
            cw = cw + jnp.where(lane8 < 128 - k, pltpu.roll(cw, 128 - k, 1), 0.0)
        cum = jnp.concatenate([cf, cw], axis=0)
        last = jnp.concatenate([cf[:, 127:128], cw[:, 0:1]], axis=0)
        e1 = jnp.exp2(cum)
        e2 = step * jnp.exp2(last - cum)
        STP[b] = step
        CUM[b] = cum
        MT[b * BLK : (b + 1) * BLK, :] = jnp.concatenate(
            [cum, e1, e2, jnp.zeros((80, 128), f32)], axis=0
        ).T

    def pre_block(b):
        r0 = b * BLK
        m = MT[r0 : r0 + 128, :]
        hi = m.astype(bf16)
        lo = (m - hi.astype(f32)).astype(bf16)
        both = jnp.concatenate([hi, lo], axis=1)
        bts = [None, None]
        for ct in (4, 5, 6, 7, 0, 1, 2, 3):
            acc = None
            for j in range(5):
                term = MX[ct, r0 + 6 + j : r0 + 6 + j + 128, :] * TAPS[j : j + 1, ct * 128 : (ct + 1) * 128]
                acc = term if acc is None else acc + term
            act = silu(acc).astype(bf16)
            if ct >= 6:
                CA[r0 : r0 + 128, (ct - 6) * 128 : (ct - 5) * 128] = act
            elif ct >= 4:
                BA[r0 : r0 + 128, (ct - 4) * 128 : (ct - 3) * 128] = act
                bts[ct - 4] = act.astype(f32).T.astype(bf16)
            else:
                INN[r0 : r0 + 128, ct * 128 : (ct + 1) * 128] = act
                if ct % 2 == 0:
                    continue
                g = ct // 2
                for d in range(2):
                    c0 = d * 512 + g * 256
                    e2x = mm(both, SPR[1, :, c0 : c0 + 256])
                    loaded = (INN[r0 : r0 + 128, g * 256 : (g + 1) * 256].astype(f32) * e2x).astype(bf16)
                    BS[b, :, c0 : c0 + 256] = mm(bts[g], loaded)
        e1x = mm(both, SPR[0])
        E1X[r0 : r0 + 128, :] = e1x
        FL[b, 0:1, 0:512] = e1x[127:128, 0:512]
        FL[b, 0:1, 512:1024] = e1x[0:1, 512:1024]

    def query_tile(h, n):
        h0 = h * 512
        p = mm(XO[h][...], WQ[pl.ds(own, HALF), n * 256 : (n + 1) * 256]) + mm(
            XP[h][...], WQ[pl.ds(oth, HALF), n * 256 : (n + 1) * 256]
        )
        qp = [(p[:, q * 128 : (q + 1) * 128] * RS[h]).astype(bf16).astype(f32) for q in range(2)]
        ms = mm(jnp.concatenate([(v * v).astype(bf16) for v in qp], axis=1), HM[...])
        for q in range(2):
            for i in range(4):
                sub = slice(i * 128, (i + 1) * 128)
                v = rotated(qp[q][sub] * lax.rsqrt(ms[sub, q * 128 : (q + 1) * 128] + EPS) * qg, h0 + i * 128)
                QM[n, h * 4 + i, q * 256 : q * 256 + 128, :] = jnp.where(lo_half, v, 0.0).astype(bf16)
                QM[n, h * 4 + i, q * 256 + 128 : q * 256 + 256, :] = jnp.where(lo_half, 0.0, v).astype(bf16)

    def gate_tile(h, n):
        h0 = h * 512
        p = mm(XO[h][...], WG[pl.ds(own, HALF), n * 256 : (n + 1) * 256]) + mm(
            XP[h][...], WG[pl.ds(oth, HALF), n * 256 : (n + 1) * 256]
        )
        for q in range(2):
            gp = (p[:, q * 128 : (q + 1) * 128] * RS[h]).astype(bf16).astype(f32)
            SG[h0 : h0 + 512, n * 256 + q * 128 : n * 256 + (q + 1) * 128] = silu(gp)

    for b in range(NB):
        steps(b)
    for i, b in enumerate((1, 2, 3, 4, 5, 6, 7, 0)):
        if i == 6:
            with jax.named_scope("w_halo"):
                for e in range(2):
                    remote(MX.at[:, 8:16, :], MXR.at[e], ms_s.at[e], ms_r.at[e], left).wait_recv()
            MX[:, 0:8, :] = jnp.where(me == 0, 0.0, MXR[0])
            MX[:, 8 + TOK : 16 + TOK, :] = jnp.where(me == nsp - 1, 0.0, MXR[1])
        (query_tile if i < 4 else gate_tile)((i // 2) % 2, i % 2)
        pre_block(b)

    fd = FL[0, 0:1, :]
    for b in range(1, NB):
        fd = fd * FL[b, 0:1, :]
    FS[...] = jnp.concatenate([fd[:, i * 128 : (i + 1) * 128] for i in range(8)], axis=0)
    FR[me] = FS[...]

    def chain_out(k):
        n0 = pl.multiple_of(k * 8, 8)
        rf = jnp.zeros((8, 512), f32)
        rb = jnp.zeros((8, 512), f32)
        for b in range(NB):
            rf = FL[b, 0:1, 0:512] * rf + BS[b, pl.ds(n0, 8), 0:512]
            z = NB - 1 - b
            rb = FL[z, 0:1, 512:1024] * rb + BS[z, pl.ds(n0, 8), 512:1024]
        return jnp.concatenate([rf, rb], axis=0).astype(bf16)

    SR[me] = chain_out(me)

    @pl.loop(1, nsp)
    def _(j):
        k = lax.rem(me + j, nsp)
        SS[k] = chain_out(k)
        remote(FS, FR.at[me], fs_s.at[k], fs_r.at[me], {"sp": k}).start()
        remote(SS.at[k], SR.at[me], ss_s.at[k], ss_r.at[me], {"sp": k}).start()

    with jax.named_scope("w_kvh"):
        for e in range(2):
            remote(KVS.at[e], KVR.at[e], hs_s.at[e], hs_r.at[e], left).wait_recv()
    for e in range(2):
        keep_kv(
            KVR[e, :, 0:128].astype(f32), KVR[e, :, 128:256].astype(f32), 0 if e == 0 else 128 + TOK
        )

    def attend(b):
        r0 = pl.multiple_of(b * BLK, BLK)
        off_l = jnp.where((me == 0) & (b == 0), 1024, 0)
        off_r = jnp.where((me == nsp - 1) & (b == NB - 1), 1024, 0)
        keep_l = g_col >= g_row + off_l
        keep_r = g_col <= g_row - off_r
        for g in range(2):
            kk = KD[g, pl.ds(r0, 384), :]
            vv = VD[g, pl.ds(r0, 384), :]
            s = lax.dot_general(QM[g, b], kk, NT, preferred_element_type=f32)
            ps, ms = [], []
            for j in range(4):
                sj = s[j * 128 : (j + 1) * 128]
                sl = jnp.where(keep_l, sj[:, 0:128], NEG)
                sm = sj[:, 128:256]
                sr = jnp.where(keep_r, sj[:, 256:384], NEG)
                sk = sink[g * 4 + j] * LOG2E
                m = jnp.max(jnp.maximum(jnp.maximum(sl, sm), sr), axis=1, keepdims=True)
                m = jnp.broadcast_to(jnp.maximum(m, sk), (128, 128))
                ps.append(jnp.concatenate([jnp.exp2(v - m).astype(bf16) for v in (sl, sm, sr)], axis=1))
                ms.append(jnp.exp2(sk - m))
            o = mm(jnp.concatenate(ps, axis=0), vv)
            res = [
                o[j * 128 : (j + 1) * 128, 0:128] / (o[j * 128 : (j + 1) * 128, 128:256] + ms[j]) for j in range(4)
            ]
            for pair in range(2):
                tile = g * 2 + pair
                AT[pl.ds(r0, 128), tile * 128 : (tile + 1) * 128] = jnp.where(
                    lo_half, res[2 * pair], res[2 * pair + 1]
                ).astype(bf16)

    def inside(b):
        r0 = pl.multiple_of(b * BLK, BLK)
        lower = g_row >= g_col
        diag = g_row == g_col
        for g in range(2):
            cm = CA[pl.ds(r0, 128), g * 128 : (g + 1) * 128]
            bm = BA[pl.ds(r0, 128), g * 128 : (g + 1) * 128]
            sc = lax.dot_general(cm, bm, NT, preferred_element_type=f32)
            for pair in range(2):
                tile = g * 2 + pair
                xt = INN[pl.ds(r0, 128), tile * 128 : (tile + 1) * 128].astype(f32)
                ws = []
                for j in range(2):
                    h = tile * 2 + j
                    dif = jnp.where(
                        lower,
                        MT[pl.ds(r0, 128), h : h + 1] - CUM[b, h : h + 1, :],
                        MT[pl.ds(r0, 128), 8 + h : 9 + h] - CUM[b, 8 + h : 9 + h, :],
                    )
                    sf, sb = STP[b, h : h + 1, :], STP[b, 8 + h : 9 + h, :]
                    st = jnp.where(diag, sf + sb, jnp.where(lower, sf, sb))
                    ws.append((sc * jnp.exp2(dif) * st).astype(bf16))
                both = jnp.concatenate(ws, axis=1)
                xx = jnp.concatenate(
                    [jnp.where(lo_half, xt, 0.0).astype(bf16), jnp.where(lo_half, 0.0, xt).astype(bf16)],
                    axis=0,
                )
                WN[pl.ds(r0, 128), tile * 128 : (tile + 1) * 128] = mm(both, xx)

    @pl.loop(0, 5)
    def _(b):
        attend(b)
        inside(b)

    with jax.named_scope("w_s"):
        for j in range(1, nsp):
            k = lax.rem(me + j, nsp)
            remote(FS, FR.at[k], fs_s.at[k], fs_r.at[k], {"sp": k}).wait_recv()
            remote(SS.at[k], SR.at[k], ss_s.at[k], ss_r.at[k], {"sp": k}).wait_recv()

    n0 = pl.multiple_of(me * 8, 8)

    def decay_row(d, which):
        return jnp.concatenate([FR[d, which * 4 + i : which * 4 + i + 1, :] for i in range(4)], axis=1)

    run = SST[0, pl.ds(n0, 8), :]
    for d in range(nsp):
        EF[d] = run
        run = decay_row(d, 0) * run + SR[d].astype(f32)[0:8]
    run = SST[1, pl.ds(n0, 8), :]
    for d in range(nsp - 1, -1, -1):
        ES[d] = jnp.concatenate([EF[d], run], axis=0).astype(bf16)
        run = decay_row(d, 1) * run + SR[d].astype(f32)[8:16]
    ER[me] = ES[me]

    @pl.loop(1, nsp)
    def _(j):
        k = lax.rem(me + j, nsp)
        remote(ES.at[k], ER.at[me], es_s.at[k], es_r.at[me], {"sp": k}).start()

    @pl.loop(5, NB)
    def _(b):
        attend(b)
        inside(b)

    with jax.named_scope("w_e"):
        for j in range(1, nsp):
            k = lax.rem(me + j, nsp)
            remote(ES.at[k], ER.at[k], es_s.at[k], es_r.at[k], {"sp": k}).wait_recv()

    @pl.loop(0, 8)
    def _(i):
        n1 = pl.multiple_of(i * 16, 16)
        ea = ER[2 * i].astype(f32)
        eb = ER[2 * i + 1].astype(f32)
        rf = jnp.concatenate([ea[0:8], eb[0:8]], axis=0)
        rb = jnp.concatenate([ea[8:16], eb[8:16]], axis=0)
        for b in range(NB):
            ENT[b, pl.ds(n1, 16), 0:512] = rf.astype(bf16)
            rf = FL[b, 0:1, 0:512] * rf + BS[b, pl.ds(n1, 16), 0:512]
            z = NB - 1 - b
            ENT[z, pl.ds(n1, 16), 512:1024] = rb.astype(bf16)
            rb = FL[z, 0:1, 512:1024] * rb + BS[z, pl.ds(n1, 16), 512:1024]

    group_mean = jnp.full((256, 256), 1.0 / 256, bf16)

    def finish(b):
        r0 = pl.multiple_of(b * BLK, BLK)
        for g in range(2):
            cm = CA[pl.ds(r0, 128), g * 128 : (g + 1) * 128]
            c0, c1 = g * 256, (g + 1) * 256
            tot = (
                WN[pl.ds(r0, 128), c0:c1]
                + mm(cm, ENT[b, :, c0:c1]) * E1X[pl.ds(r0, 128), c0:c1]
                + mm(cm, ENT[b, :, 512 + c0 : 512 + c1]) * E1X[pl.ds(r0, 128), 512 + c0 : 512 + c1]
            )
            gated = tot * SG[pl.ds(r0, 128), c0:c1]
            ms = mm((gated * gated).astype(bf16), group_mean)
            AT[pl.ds(r0, 128), 512 + c0 : 512 + c1] = (
                gated * lax.rsqrt(ms + EPS) * ggain[0:1, c0:c1]
            ).astype(bf16)

    with jax.named_scope("w_wo"):
        third[2].wait()
        third[3].wait()
    other = pl.multiple_of((1 - t) * 512, 512)
    mine = pl.multiple_of(t * 512, 512)
    pc = []
    oc = []

    @pl.loop(0, 4)
    def _(i):
        finish((1 - t) * 4 + i)

    for n in range(8):
        dst = (XO0, XP0)[n // 4]
        c0 = (n % 4) * 256
        dst[:, c0 : c0 + 256] = mm(AT[pl.ds(other, 512), :], WO[:, n * 256 : (n + 1) * 256]).astype(bf16)
        if n % 2 == 1:
            c = remote(
                dst.at[:, c0 - 256 : c0 + 256], PR.at[:, (n - 1) * 256 : (n + 1) * 256],
                ps_s.at[n // 2], ps_r.at[n // 2], peer,
            )
            c.start()
            pc.append(c)

    @pl.loop(0, 4)
    def _(i):
        finish(t * 4 + i)

    for n in range(8):
        dst = (XO1, XP1)[n // 4]
        c0 = (n % 4) * 256
        p = mm(AT[pl.ds(mine, 512), :], WO[:, n * 256 : (n + 1) * 256]).astype(bf16).astype(f32)
        if n % 2 == 0:
            with jax.named_scope(f"w_p{n}"):
                pc[n // 2].wait_recv()
        dst[:, c0 : c0 + 256] = (p + PR[:, n * 256 : (n + 1) * 256].astype(f32)).astype(bf16)
        if n % 2 == 1:
            c = pltpu.make_async_copy(
                dst.at[:, c0 - 256 : c0 + 256], out.at[:, (n - 1) * 256 : (n + 1) * 256], osem.at[n // 2]
            )
            c.start()
            oc.append(c)

    with jax.named_scope("w_snd"):
        for c in xc + sends + pc:
            c.wait_send()

        @pl.loop(1, nsp)
        def _(j):
            k = lax.rem(me + j, nsp)
            remote(FS, FR.at[me], fs_s.at[k], fs_r.at[me], {"sp": k}).wait_send()
            remote(SS.at[k], SR.at[me], ss_s.at[k], ss_r.at[me], {"sp": k}).wait_send()
            remote(ES.at[k], ER.at[me], es_s.at[k], es_r.at[me], {"sp": k}).wait_send()

        for c in oc:
            c.wait()


def tables(blocks):
    freq = 10000.0 ** (-(np.arange(128) % 32) / 32.0)
    a = np.arange(blocks)[:, None] * 128.0 * freq[None, :]
    r = np.arange(128)[:, None] * freq[None, :]
    return (
        np.stack([np.cos(a), np.sin(a)]).astype(np.float32),
        np.stack([np.cos(r), np.sin(r)]).astype(np.float32),
    )


def local(
    nsp, inputs, mix_gain, w_query, w_key, w_value, query_gain, key_gain, sink_logit, w_inner, w_bmat, w_cmat,
    w_gate, w_step, conv_inner, conv_bmat, conv_cmat, step_bias, decay_rate, decay_offset, start_state,
    group_gain, w_out_attn, w_out_state,
):
    wst = jnp.transpose(w_step, (1, 2, 0)).reshape(16, D)
    off = jnp.transpose(decay_offset, (1, 2, 0)).reshape(16, TOK)
    tabs, rows = tables(nsp * NB)
    hbm = pl.BlockSpec(memory_space=pl.ANY)
    vm = pl.BlockSpec(memory_space=pltpu.VMEM)
    sm = pl.BlockSpec(memory_space=pltpu.SMEM)
    V = pltpu.VMEM
    dma = pltpu.SemaphoreType.DMA
    return pl.pallas_call(
        lambda *refs: kernel(nsp, *refs),
        name="layer",
        out_shape=jax.ShapeDtypeStruct((TOK // 2, D), bf16),
        in_specs=[hbm, vm, hbm, hbm, hbm, hbm, hbm, hbm, hbm, vm, vm, vm, sm, vm, vm, vm, sm, sm, vm, hbm, vm, hbm, hbm, hbm, hbm],
        out_specs=hbm,
        scratch_shapes=[
            V((512, HALF), bf16), V((512, HALF), bf16), V((512, HALF), bf16), V((512, HALF), bf16),
            V((2, 512, 128), f32),
            V((D, 512), bf16), V((D, 256), bf16), V((D, 512), bf16), V((D, 512), bf16), V((D, 512), bf16),
            V((1024, D), bf16), V((128, D), bf16),
            V((2, NB, 512, 128), bf16), V((2, TOK + 256, 128), bf16), V((2, TOK + 256, 256), bf16),
            V((2, 128, 256), bf16), V((2, 128, 256), bf16),
            V((8, TOK + 16, 128), f32), V((2, 8, 8, 128), f32), V((TOK, 512), f32), V((8, 1024), f32),
            V((TOK, 128), f32), V((TOK, 128), f32),
            V((NB, 16, 128), f32), V((NB, 16, 128), f32), V((TOK, 128), f32),
            V((TOK, 512), bf16), V((TOK, 256), bf16), V((TOK, 256), bf16),
            V((TOK, 1024), f32), V((NB, 8, 1024), f32), V((NB, 128, 1024), f32),
            V((nsp, 16, 512), bf16), V((nsp, 16, 512), bf16), V((8, 128), f32), V((nsp, 8, 128), f32),
            V((nsp, 16, 512), bf16), V((nsp, 16, 512), bf16), V((nsp, 8, 512), f32),
            V((NB, 128, 1024), bf16),
            V((TOK, 512), f32), V((TOK, 1024), bf16), V((512, D), bf16), V((2, 128, 512), f32), V((2, 256, 1024), bf16),
            V((256, 256), bf16), V((2, 512, 128), f32), V((2, 8, 128), f32), V((2, 128, 128), f32),
            dma((5,)), dma((14,)), dma((2,)), dma((2,)), dma((2,)), dma((2,)), dma((2,)), dma((2,)),
            dma((nsp,)), dma((nsp,)), dma((nsp,)), dma((nsp,)), dma((nsp,)), dma((nsp,)), dma((4,)), dma((4,)), dma((4,)),
        ],
        compiler_params=pltpu.CompilerParams(
            collective_id=0, has_side_effects=True, vmem_limit_bytes=56 * 1024 * 1024
        ),
    )(
        inputs, mix_gain.reshape(1, D), w_query, w_key, w_value, w_inner, w_bmat, w_cmat, w_gate, wst,
        query_gain.reshape(1, 64), key_gain.reshape(1, 64), sink_logit, conv_inner, conv_bmat, conv_cmat,
        step_bias, decay_rate, off, start_state.reshape(2, 512, 128),
        group_gain.reshape(1, 512), w_out_attn, w_out_state, jnp.asarray(tabs), jnp.asarray(rows),
    )


def solution(mesh):
    nsp = mesh.shape["sp"]
    return jax.shard_map(
        lambda *args: local(nsp, *args),
        mesh=mesh,
        in_specs=(
            P(("fs", "sp"), "tp"), P(), P(None, "tp"), P(None, "tp"), P(None, "tp"), P(), P(), P("tp"),
            P(None, "tp"), P(None, "tp"), P(None, "tp"), P(None, "tp"), P(None, None, "tp"),
            P(None, "tp"), P(None, "tp"), P(None, "tp"), P(None, "tp"), P(None, "tp"),
            P("sp", None, "tp"), P("fs", "tp", None, None), P("tp"), P("tp", None), P("tp", None),
        ),
        out_specs=P(("fs", "sp", "tp"), None),
        check_vma=False,
    )
```

```python
import math

import jax
import jax.numpy as jnp
import numpy as np
from jax import lax
from jax.experimental import pallas as pl
from jax.experimental.pallas import tpu as pltpu
from jax.sharding import PartitionSpec as P

D = 2048
HALF = 1024
TOK = 1024
BLK = 128
NB = 8
EPS = 1e-06
LOG2E = math.log2(math.e)
NEG = -1e30
MESH = pl.DeviceIdType.MESH
NT = (((1,), (1,)), ((), ()))
f32 = jnp.float32
bf16 = jnp.bfloat16


def iota(shape, dim):
    return lax.broadcasted_iota(jnp.int32, shape, dim)


def mm(a, b):
    return jnp.dot(a, b, preferred_element_type=f32)


def silu(v):
    h = 0.5 * v
    return h + h * jnp.tanh(h)


def kernel(
    nsp,
    x, gain_, wq, wk, wv, wi, wb, wc, wg, wst_, qgain_, kgain_, sink_, ci_, cb_, cc_,
    bias_, rate_, off_, start, ggain_, woa, wos, tabs, rows,
    out,
    XO0, XO1, XP0, XP1, RS, WQ, WKV, WI, WBC, WG, WO, WST, QM, KD, VD, KVS, KVR, MX, MXR, SG, TAPS,
    COS, SIN, STP, CUM, MT, INN, BA, CA, E1X, FL, BS, SS, SR, FS, FR, ES, ER, EF, ENT,
    WN, AT, PR, SST, SPR, HM, STV, TBV, RWV,
    gain, wst, qgain, kgain, sink, ci, cb, cc, bias, rate, off, ggain,
    asem, lsem, wsem, xs_s, xs_r, hs_s, hs_r, ms_s, ms_r, ss_s, ss_r, fs_s, fs_r, es_s, es_r, ps_s, ps_r,
):
    me = lax.axis_index("sp")
    t = lax.axis_index("tp")
    peer = {"tp": 1 - t}
    left = {"sp": lax.rem(me + nsp - 1, nsp)}
    right = {"sp": lax.rem(me + 1, nsp)}
    XO, XP = (XO0, XO1), (XP0, XP1)

    def remote(src, dst, s, r, dev):
        return pltpu.make_async_remote_copy(
            src_ref=src, dst_ref=dst, send_sem=s, recv_sem=r, device_id=dev, device_id_type=MESH
        )

    barrier = pltpu.get_barrier_semaphore()
    pl.semaphore_signal(barrier, inc=1, device_id=peer, device_id_type=MESH)
    for j in range(1, nsp):
        pl.semaphore_signal(
            barrier, inc=1, device_id={"sp": lax.rem(me + j, nsp)}, device_id_type=MESH
        )

    own = pl.multiple_of(t * HALF, HALF)
    oth = pl.multiple_of((1 - t) * HALF, HALF)
    xl = [pltpu.make_async_copy(x.at[h * 512 : (h + 1) * 512, :], XO[h], lsem.at[h]) for h in range(2)]
    small = [
        pltpu.make_async_copy(start, STV, lsem.at[2]),
        pltpu.make_async_copy(tabs.at[:, pl.ds(pl.multiple_of(me * NB, NB), NB), :], TBV, lsem.at[3]),
        pltpu.make_async_copy(rows, RWV, lsem.at[4]),
    ]
    pieces = [(wk, WKV, 0, 128), (wv, WKV, 128, 128), (wi, WI, 0, 512), (wb, WBC, 0, 256), (wc, WBC, 256, 256)]
    first = [
        pltpu.make_async_copy(w.at[pl.ds(own, HALF), :], d.at[pl.ds(own, HALF), c0 : c0 + n], wsem.at[i])
        for i, (w, d, c0, n) in enumerate(pieces)
    ]
    second = [
        pltpu.make_async_copy(w.at[pl.ds(oth, HALF), :], d.at[pl.ds(oth, HALF), c0 : c0 + n], wsem.at[5 + i])
        for i, (w, d, c0, n) in enumerate(pieces)
    ]
    third = [
        pltpu.make_async_copy(wq, WQ, wsem.at[10]),
        pltpu.make_async_copy(wg, WG, wsem.at[11]),
        pltpu.make_async_copy(woa, WO.at[0:512], wsem.at[12]),
        pltpu.make_async_copy(wos, WO.at[512:1024], wsem.at[13]),
    ]
    args = [
        pltpu.make_async_copy(a, b, asem.at[i])
        for i, (a, b) in enumerate(
            [
                (gain_, gain), (wst_, wst), (qgain_, qgain), (kgain_, kgain), (sink_, sink), (ci_, ci), (cb_, cb),
                (cc_, cc), (bias_, bias), (rate_, rate), (off_, off), (ggain_, ggain),
            ]
        )
    ]
    for c in [args[0], xl[0], args[1]] + first[:2] + args[2:]:
        c.start()

    lane = iota((1, 128), 1)
    lo_half = lane < 64
    first_part = lax.rem(lane, 64) < 32
    g_row, g_col = iota((128, 128), 0), iota((128, 128), 1)
    ones_lanes = jnp.ones((128, 128), bf16)
    HM[...] = jnp.where(iota((256, 256), 0) // 64 == iota((256, 256), 1) // 64, 1.0 / 64, 0.0).astype(bf16)
    WST[...] = jnp.zeros((128, D), bf16)

    def scale(ref, at, h, begin):
        g = gain[0:1, pl.ds(at, HALF)]
        for i in range(8):
            r = i * 64
            v = ref[r : r + 64, :].astype(f32)
            ref[r : r + 64, :] = (v * g).astype(bf16)
            ss = jnp.broadcast_to(jnp.sum(v * v, axis=1, keepdims=True), (64, 128))
            if begin:
                RS[h, r : r + 64, :] = ss
            else:
                RS[h, r : r + 64, :] = lax.rsqrt((RS[h, r : r + 64, :] + ss) * (1.0 / D) + EPS)

    for c in first[2:] + [xl[1]] + small:
        c.start()
    mixed_tiles = [(WI, 0), (WI, 256), (WBC, 0), (WBC, 256)]

    def part_one(h):
        rows_ = slice(h * 512, (h + 1) * 512)
        xs = XO[h][...]
        WN[rows_, 0:256] = mm(xs, WKV[pl.ds(own, HALF), :])
        WN[rows_, 256:384] = lax.dot_general(xs, WST[:, pl.ds(own, HALF)], NT, preferred_element_type=f32)
        if h == 0:
            for c in first[2:]:
                c.wait()
        for n, (w, c0) in enumerate(mixed_tiles):
            E1X[rows_, n * 256 : (n + 1) * 256] = mm(xs, w[pl.ds(own, HALF), c0 : c0 + 256])

    with jax.named_scope("w_xl0"):
        xl[0].wait()
        for c in args[:2]:
            c.wait()
    WST[0:16, :] = wst[...]
    for c in second + third:
        c.start()
    scale(XO[0], own, 0, True)
    with jax.named_scope("w_f0"):
        first[0].wait()
        first[1].wait()
    with jax.named_scope("w_barrier"):
        pl.semaphore_wait(barrier, nsp)
    xc = []
    for h in range(2):
        c = remote(x.at[h * 512 : (h + 1) * 512, :], XP[h], xs_s.at[h], xs_r.at[h], peer)
        c.start()
        xc.append(c)
    part_one(0)
    with jax.named_scope("w_xl1"):
        xl[1].wait()
        for c in small + args[2:]:
            c.wait()
    TAPS[0:5, 0:512] = ci[...].astype(f32)
    TAPS[0:5, 512:768] = cb[...].astype(f32)
    TAPS[0:5, 768:1024] = cc[...].astype(f32)
    qg = jnp.concatenate([qgain[...], qgain[...]], axis=1) * (LOG2E / 8.0)
    kg = jnp.concatenate([kgain[...], kgain[...]], axis=1)
    scale(XO[1], own, 1, True)
    part_one(1)

    for d in range(2):
        for q in range(4):
            SST[d, :, q * 128 : (q + 1) * 128] = STV[d, q * 128 : (q + 1) * 128, :].T
    sign = jnp.where(first_part, -1.0, 1.0).astype(f32)
    for b in range(NB):
        ac, as_ = TBV[0, b : b + 1, :], TBV[1, b : b + 1, :]
        COS[b * BLK : (b + 1) * BLK, :] = ac * RWV[0] - as_ * RWV[1]
        SIN[b * BLK : (b + 1) * BLK, :] = (as_ * RWV[0] + ac * RWV[1]) * sign
    for d in range(2):
        ex_row, ex_col = lax.rem(iota((256, 1024), 0), 128), iota((256, 1024), 1) // 64
        SPR[d] = jnp.where(ex_row == ex_col + 16 * (d + 1), 1.0, 0.0).astype(bf16)

    def rotated(n, r0):
        partner = jnp.where(first_part, pltpu.roll(n, 96, 1), pltpu.roll(n, 32, 1))
        return n * COS[r0 : r0 + 128, :] + partner * SIN[r0 : r0 + 128, :]

    def keep_kv(kb, vb, f0):
        kr, vr = pltpu.roll(kb, 64, 1), pltpu.roll(vb, 64, 1)
        KD[0, f0 : f0 + 128, :] = jnp.where(lo_half, kb, kr).astype(bf16)
        KD[1, f0 : f0 + 128, :] = jnp.where(lo_half, kr, kb).astype(bf16)
        VD[0, f0 : f0 + 128, 0:128] = jnp.where(lo_half, vb, vr).astype(bf16)
        VD[1, f0 : f0 + 128, 0:128] = jnp.where(lo_half, vr, vb).astype(bf16)
        VD[0, f0 : f0 + 128, 128:256] = ones_lanes
        VD[1, f0 : f0 + 128, 128:256] = ones_lanes

    sends = []

    def part_two(h):
        h0 = h * 512
        rows_ = slice(h0, h0 + 512)
        xs = XP[h][...]
        for n, (w, c0) in enumerate(mixed_tiles):
            p = mm(xs, w[pl.ds(oth, HALF), c0 : c0 + 256])
            for q in range(2):
                ct = 2 * n + q
                MX[ct, 8 + h0 : 8 + h0 + 512, :] = (
                    ((p[:, q * 128 : (q + 1) * 128] + E1X[rows_, ct * 128 : (ct + 1) * 128]) * RS[h])
                    .astype(bf16)
                    .astype(f32)
                )
        kv = mm(xs, WKV[pl.ds(oth, HALF), :])
        sp_ = lax.dot_general(xs, WST[:, pl.ds(oth, HALF)], NT, preferred_element_type=f32)
        for i in range(4):
            sub = slice(i * 128, (i + 1) * 128)
            STP[h * 4 + i] = ((sp_[sub] + WN[h0 + i * 128 : h0 + (i + 1) * 128, 256:384]) * RS[h, sub, :]).T[0:16]
        kp = ((kv[:, 0:128] + WN[rows_, 0:128]) * RS[h]).astype(bf16).astype(f32)
        vb = ((kv[:, 128:256] + WN[rows_, 128:256]) * RS[h]).astype(bf16).astype(f32)
        ms = mm((kp * kp).astype(bf16), HM[0:128, 0:128])
        for i in range(4):
            r0 = h0 + i * 128
            sub = slice(i * 128, (i + 1) * 128)
            k = rotated(kp[sub] * lax.rsqrt(ms[sub] + EPS) * kg, r0)
            kb = k.astype(bf16).astype(f32)
            keep_kv(kb, vb[sub], r0 + 128)
            if r0 == 0 or r0 == 896:
                KVS[h, :, 0:128] = kb.astype(bf16)
                KVS[h, :, 128:256] = vb[sub].astype(bf16)
        dev = left if h == 0 else right
        mrow = 8 if h == 0 else TOK
        c = remote(MX.at[:, mrow : mrow + 8, :], MXR.at[1 - h], ms_s.at[h], ms_r.at[1 - h], dev)
        c.start()
        sends.append(c)
        c = remote(KVS.at[h], KVR.at[1 - h], hs_s.at[h], hs_r.at[1 - h], dev)
        c.start()
        sends.append(c)

    row16 = iota((16, 128), 0)
    bias_c = jnp.zeros((16, 128), f32)
    rate_c = jnp.zeros((16, 128), f32)
    for r in range(16):
        bias_c = jnp.where(row16 == r, bias[r // 8, r % 8], bias_c)
        rate_c = jnp.where(row16 == r, rate[r // 8, r % 8], rate_c)
    lane8 = iota((8, 128), 1)

    def steps(b):
        v = STP[b] + bias_c
        step = jnp.maximum(v, 0.0) + jnp.log1p(jnp.exp(-jnp.abs(v)))
        la = (-rate_c * step + off[:, b * BLK : (b + 1) * BLK]) * LOG2E
        cf, cw = la[0:8], la[8:16]
        for k in (1, 2, 4, 8, 16, 32, 64):
            cf = cf + jnp.where(lane8 >= k, pltpu.roll(cf, k, 1), 0.0)
            cw = cw + jnp.where(lane8 < 128 - k, pltpu.roll(cw, 128 - k, 1), 0.0)
        cum = jnp.concatenate([cf, cw], axis=0)
        last = jnp.concatenate([cf[:, 127:128], cw[:, 0:1]], axis=0)
        e1 = jnp.exp2(cum)
        e2 = step * jnp.exp2(last - cum)
        STP[b] = step
        CUM[b] = cum
        MT[b * BLK : (b + 1) * BLK, :] = jnp.concatenate(
            [cum, e1, e2, jnp.zeros((80, 128), f32)], axis=0
        ).T

    def pre_block(b):
        r0 = b * BLK
        bts = [None, None]
        for ct in (4, 5, 6, 7, 0, 1, 2, 3):
            acc = None
            for j in range(5):
                term = MX[ct, r0 + 6 + j : r0 + 6 + j + 128, :] * TAPS[j : j + 1, ct * 128 : (ct + 1) * 128]
                acc = term if acc is None else acc + term
            act = silu(acc).astype(bf16)
            if ct >= 6:
                CA[r0 : r0 + 128, (ct - 6) * 128 : (ct - 5) * 128] = act
            elif ct >= 4:
                BA[r0 : r0 + 128, (ct - 4) * 128 : (ct - 3) * 128] = act
                bts[ct - 4] = act.astype(f32).T.astype(bf16)
            else:
                INN[r0 : r0 + 128, ct * 128 : (ct + 1) * 128] = act
                if ct % 2 == 0:
                    continue
                g = ct // 2
                for d in range(2):
                    c0 = d * 512 + g * 256
                    loaded = (
                        INN[r0 : r0 + 128, g * 256 : (g + 1) * 256].astype(f32) * BS[b, :, c0 : c0 + 256]
                    ).astype(bf16)
                    BS[b, :, c0 : c0 + 256] = mm(bts[g], loaded)

    def spread(h):
        m = MT[h * 512 : (h + 1) * 512, :]
        hi = m.astype(bf16)
        lo = (m - hi.astype(f32)).astype(bf16)
        both = jnp.concatenate([hi, lo], axis=1)
        for n in range(4):
            c = slice(n * 256, (n + 1) * 256)
            e1x = mm(both, SPR[0, :, c])
            E1X[h * 512 : (h + 1) * 512, c] = e1x
            e2x = mm(both, SPR[1, :, c])
            for i in range(4):
                r = i * 128 + (127 if n < 2 else 0)
                FL[h * 4 + i, 0:1, c] = e1x[r : r + 1, :]
                BS[h * 4 + i, :, c] = e2x[i * 128 : (i + 1) * 128]

    def query(h):
        h0 = h * 512
        p = mm(XO[h][...], WQ[pl.ds(own, HALF), :]) + mm(XP[h][...], WQ[pl.ds(oth, HALF), :])
        qp = [(p[:, q * 128 : (q + 1) * 128] * RS[h]).astype(bf16).astype(f32) for q in range(4)]
        for n in range(2):
            ms = mm(jnp.concatenate([(v * v).astype(bf16) for v in qp[2 * n : 2 * n + 2]], axis=1), HM[...])
            for q in range(2):
                for i in range(4):
                    sub = slice(i * 128, (i + 1) * 128)
                    v = qp[2 * n + q][sub] * lax.rsqrt(ms[sub, q * 128 : (q + 1) * 128] + EPS) * qg
                    v = rotated(v, h0 + i * 128)
                    QM[n, h * 4 + i, q * 256 : q * 256 + 128, :] = jnp.where(lo_half, v, 0.0).astype(bf16)
                    QM[n, h * 4 + i, q * 256 + 128 : q * 256 + 256, :] = jnp.where(lo_half, 0.0, v).astype(bf16)

    def gate_tile(h, n):
        h0 = h * 512
        p = mm(XO[h][...], WG[pl.ds(own, HALF), n * 256 : (n + 1) * 256]) + mm(
            XP[h][...], WG[pl.ds(oth, HALF), n * 256 : (n + 1) * 256]
        )
        for q in range(2):
            gp = (p[:, q * 128 : (q + 1) * 128] * RS[h]).astype(bf16).astype(f32)
            SG[h0 : h0 + 512, n * 256 + q * 128 : n * 256 + (q + 1) * 128] = silu(gp)

    with jax.named_scope("w_x0"):
        xc[0].wait_recv()
        for c in second:
            c.wait()
    scale(XP[0], oth, 0, False)
    part_two(0)
    with jax.named_scope("w_x1"):
        xc[1].wait_recv()
        third[0].wait()
        third[1].wait()
    scale(XP[1], oth, 1, False)
    part_two(1)
    for b in range(4):
        steps(b)
    spread(0)
    query(0)
    for b in (1, 2):
        pre_block(b)
    for b in range(4, 8):
        steps(b)
    spread(1)
    query(1)
    for b in (3, 4, 5, 6):
        pre_block(b)
    with jax.named_scope("w_halo"):
        for e in range(2):
            remote(MX.at[:, 8:16, :], MXR.at[e], ms_s.at[e], ms_r.at[e], left).wait_recv()
    MX[:, 0:8, :] = jnp.where(me == 0, 0.0, MXR[0])
    MX[:, 8 + TOK : 16 + TOK, :] = jnp.where(me == nsp - 1, 0.0, MXR[1])
    for b in (7, 0):
        pre_block(b)

    fd = FL[0, 0:1, :]
    for b in range(1, NB):
        fd = fd * FL[b, 0:1, :]
    FS[...] = jnp.concatenate([fd[:, i * 128 : (i + 1) * 128] for i in range(8)], axis=0)
    FR[me] = FS[...]

    def chain_out(k):
        n0 = pl.multiple_of(k * 8, 8)
        rf = jnp.zeros((8, 512), f32)
        rb = jnp.zeros((8, 512), f32)
        for b in range(NB):
            rf = FL[b, 0:1, 0:512] * rf + BS[b, pl.ds(n0, 8), 0:512]
            z = NB - 1 - b
            rb = FL[z, 0:1, 512:1024] * rb + BS[z, pl.ds(n0, 8), 512:1024]
        return jnp.concatenate([rf, rb], axis=0).astype(bf16)

    SR[me] = chain_out(me)

    @pl.loop(1, nsp)
    def _(j):
        k = lax.rem(me + j, nsp)
        SS[k] = chain_out(k)
        remote(FS, FR.at[me], fs_s.at[k], fs_r.at[me], {"sp": k}).start()
        remote(SS.at[k], SR.at[me], ss_s.at[k], ss_r.at[me], {"sp": k}).start()

    with jax.named_scope("w_kvh"):
        for e in range(2):
            remote(KVS.at[e], KVR.at[e], hs_s.at[e], hs_r.at[e], left).wait_recv()
        for c in sends:
            c.wait_send()
    for e in range(2):
        keep_kv(
            KVR[e, :, 0:128].astype(f32), KVR[e, :, 128:256].astype(f32), 0 if e == 0 else 128 + TOK
        )

    def attend(b):
        r0 = pl.multiple_of(b * BLK, BLK)
        off_l = jnp.where((me == 0) & (b == 0), 1024, 0)
        off_r = jnp.where((me == nsp - 1) & (b == NB - 1), 1024, 0)
        keep_l = g_col >= g_row + off_l
        keep_r = g_col <= g_row - off_r
        low, high = [], []
        for z in range(2):
            row, col = iota((64, 128), 0) + z * 64, iota((64, 128), 1)
            low.append(col >= row + off_l)
            high.append(col <= row - off_r)
        for g in range(2):
            s = lax.dot_general(QM[g, b], KD[g, pl.ds(r0, 384), :], NT, preferred_element_type=f32)
            for kt in range(3):
                MX[g * 3 + kt, 0:512, :] = s[:, kt * 128 : (kt + 1) * 128]
        for g in range(2):
            for j in range(4):
                sk = sink[g * 4 + j] * LOG2E
                for z in range(2):
                    r = j * 128 + z * 64
                    sl = jnp.where(low[z], MX[g * 3, r : r + 64, :], NEG)
                    sm = MX[g * 3 + 1, r : r + 64, :]
                    sr = jnp.where(high[z], MX[g * 3 + 2, r : r + 64, :], NEG)
                    m = jnp.max(jnp.maximum(jnp.maximum(sl, sm), sr), axis=1, keepdims=True)
                    m = jnp.broadcast_to(jnp.maximum(m, sk), (64, 128))
                    WI[g * 512 + r : g * 512 + r + 64, 0:128] = jnp.exp2(sl - m).astype(bf16)
                    WI[g * 512 + r : g * 512 + r + 64, 128:256] = jnp.exp2(sm - m).astype(bf16)
                    WI[g * 512 + r : g * 512 + r + 64, 256:384] = jnp.exp2(sr - m).astype(bf16)
                    COS[g * 512 + r : g * 512 + r + 64, :] = jnp.exp2(sk - m)
            o = mm(WI[g * 512 : (g + 1) * 512, 0:384], VD[g, pl.ds(r0, 384), :])
            for pair in range(2):
                res = []
                for j in (2 * pair, 2 * pair + 1):
                    sub = slice(j * 128, (j + 1) * 128)
                    res.append(o[sub, 0:128] / (o[sub, 128:256] + COS[g * 512 + j * 128 : g * 512 + (j + 1) * 128, :]))
                tile = g * 2 + pair
                AT[pl.ds(r0, 128), tile * 128 : (tile + 1) * 128] = jnp.where(
                    lo_half, res[0], res[1]
                ).astype(bf16)

    def inside(b):
        r0 = pl.multiple_of(b * BLK, BLK)
        for g in range(2):
            cm = CA[pl.ds(r0, 128), g * 128 : (g + 1) * 128]
            bm = BA[pl.ds(r0, 128), g * 128 : (g + 1) * 128]
            sc = lax.dot_general(cm, bm, NT, preferred_element_type=f32)
            for pair in range(2):
                tile = g * 2 + pair
                xt = INN[pl.ds(r0, 128), tile * 128 : (tile + 1) * 128].astype(f32)
                for j in range(2):
                    h = tile * 2 + j
                    for z in range(2):
                        row, col = iota((64, 128), 0) + z * 64, iota((64, 128), 1)
                        rz = pl.multiple_of(r0 + z * 64, 64)
                        dif = jnp.where(
                            row >= col,
                            MT[pl.ds(rz, 64), h : h + 1] - CUM[b, h : h + 1, :],
                            MT[pl.ds(rz, 64), 8 + h : 9 + h] - CUM[b, 8 + h : 9 + h, :],
                        )
                        sf, sb = STP[b, h : h + 1, :], STP[b, 8 + h : 9 + h, :]
                        st = jnp.where(row == col, sf + sb, jnp.where(row >= col, sf, sb))
                        WBC[tile * 128 + z * 64 : tile * 128 + z * 64 + 64, j * 128 : (j + 1) * 128] = (
                            sc[z * 64 : z * 64 + 64] * jnp.exp2(dif) * st
                        ).astype(bf16)
                xx = jnp.concatenate(
                    [jnp.where(lo_half, xt, 0.0).astype(bf16), jnp.where(lo_half, 0.0, xt).astype(bf16)],
                    axis=0,
                )
                WN[pl.ds(r0, 128), tile * 128 : (tile + 1) * 128] = mm(WBC[tile * 128 : (tile + 1) * 128, 0:256], xx)

    @pl.loop(0, 5)
    def _(b):
        attend(b)
        inside(b)

    with jax.named_scope("w_s"):
        for j in range(1, nsp):
            k = lax.rem(me + j, nsp)
            remote(FS, FR.at[k], fs_s.at[k], fs_r.at[k], {"sp": k}).wait_recv()
            remote(SS.at[k], SR.at[k], ss_s.at[k], ss_r.at[k], {"sp": k}).wait_recv()

    n0 = pl.multiple_of(me * 8, 8)

    def decay_row(d, which):
        return jnp.concatenate([FR[d, which * 4 + i : which * 4 + i + 1, :] for i in range(4)], axis=1)

    run = SST[0, pl.ds(n0, 8), :]
    for d in range(nsp):
        EF[d] = run
        run = decay_row(d, 0) * run + SR[d].astype(f32)[0:8]
    run = SST[1, pl.ds(n0, 8), :]
    for d in range(nsp - 1, -1, -1):
        ES[d] = jnp.concatenate([EF[d], run], axis=0).astype(bf16)
        run = decay_row(d, 1) * run + SR[d].astype(f32)[8:16]
    ER[me] = ES[me]

    @pl.loop(1, nsp)
    def _(j):
        k = lax.rem(me + j, nsp)
        remote(ES.at[k], ER.at[me], es_s.at[k], es_r.at[me], {"sp": k}).start()

    @pl.loop(5, NB)
    def _(b):
        attend(b)
        inside(b)

    with jax.named_scope("c_gate"):
        for h in range(2):
            for n in range(2):
                gate_tile(h, n)

    with jax.named_scope("w_e"):
        for j in range(1, nsp):
            k = lax.rem(me + j, nsp)
            remote(ES.at[k], ER.at[k], es_s.at[k], es_r.at[k], {"sp": k}).wait_recv()

    @pl.loop(0, 8)
    def _(i):
        n1 = pl.multiple_of(i * 16, 16)
        ea = ER[2 * i].astype(f32)
        eb = ER[2 * i + 1].astype(f32)
        rf = jnp.concatenate([ea[0:8], eb[0:8]], axis=0)
        rb = jnp.concatenate([ea[8:16], eb[8:16]], axis=0)
        for b in range(NB):
            ENT[b, pl.ds(n1, 16), 0:512] = rf.astype(bf16)
            rf = FL[b, 0:1, 0:512] * rf + BS[b, pl.ds(n1, 16), 0:512]
            z = NB - 1 - b
            ENT[z, pl.ds(n1, 16), 512:1024] = rb.astype(bf16)
            rb = FL[z, 0:1, 512:1024] * rb + BS[z, pl.ds(n1, 16), 512:1024]

    group_mean = jnp.full((256, 256), 1.0 / 256, bf16)

    def finish(b0):
        for g in range(2):
            c0, c1 = g * 256, (g + 1) * 256
            gated = []
            for i in range(4):
                b = b0 + i
                r0 = pl.multiple_of(b * BLK, BLK)
                cm = CA[pl.ds(r0, 128), g * 128 : (g + 1) * 128]
                tot = (
                    WN[pl.ds(r0, 128), c0:c1]
                    + mm(cm, ENT[b, :, c0:c1]) * E1X[pl.ds(r0, 128), c0:c1]
                    + mm(cm, ENT[b, :, 512 + c0 : 512 + c1]) * E1X[pl.ds(r0, 128), 512 + c0 : 512 + c1]
                )
                gated.append(tot * SG[pl.ds(r0, 128), c0:c1])
            ms = mm(jnp.concatenate([(v * v).astype(bf16) for v in gated], axis=0), group_mean)
            for i in range(4):
                r0 = pl.multiple_of((b0 + i) * BLK, BLK)
                AT[pl.ds(r0, 128), 512 + c0 : 512 + c1] = (
                    gated[i] * lax.rsqrt(ms[i * 128 : (i + 1) * 128] + EPS) * ggain[0:1, c0:c1]
                ).astype(bf16)

    with jax.named_scope("w_wo"):
        third[2].wait()
        third[3].wait()
    other = pl.multiple_of((1 - t) * 512, 512)
    mine = pl.multiple_of(t * 512, 512)
    pc = []

    with jax.named_scope("c_fin0"):
        finish((1 - t) * 4)

    for n in range(4):
        dst = (XO0, XP0)[n // 2].at[:, (n % 2) * 512 : (n % 2) * 512 + 512]
        cols = slice(n * 512, (n + 1) * 512)
        dst[...] = mm(AT[pl.ds(other, 512), :], WO[:, cols]).astype(bf16)
        c = remote(dst, PR.at[:, cols], ps_s.at[n], ps_r.at[n], peer)
        c.start()
        pc.append(c)

    with jax.named_scope("c_fin1"):
        finish(t * 4)

    def own_tile(n):
        dst = (XO1, XP1)[n // 4]
        c0 = (n % 4) * 256
        dst[:, c0 : c0 + 256] = mm(AT[pl.ds(mine, 512), :], WO[:, n * 256 : (n + 1) * 256]).astype(bf16)

    def sum_tile(n):
        own_part = (XO1, XP1)[n // 4][:, (n % 4) * 256 : (n % 4) * 256 + 256].astype(f32)
        out[:, n * 256 : (n + 1) * 256] = (own_part + PR[:, n * 256 : (n + 1) * 256].astype(f32)).astype(bf16)

    with jax.named_scope("c_out1"):
        for n in range(3):
            own_tile(n)
    with jax.named_scope("w_p"):
        for c in pc:
            c.wait_recv()
    with jax.named_scope("c_out2"):
        for n in range(3, 8):
            p = mm(AT[pl.ds(mine, 512), :], WO[:, n * 256 : (n + 1) * 256]).astype(bf16).astype(f32)
            out[:, n * 256 : (n + 1) * 256] = (p + PR[:, n * 256 : (n + 1) * 256].astype(f32)).astype(bf16)
            if n < 6:
                sum_tile(n - 3)

    with jax.named_scope("w_snd"):
        for c in xc + pc:
            c.wait_send()

        @pl.loop(1, nsp)
        def _(j):
            k = lax.rem(me + j, nsp)
            remote(FS, FR.at[me], fs_s.at[k], fs_r.at[me], {"sp": k}).wait_send()
            remote(SS.at[k], SR.at[me], ss_s.at[k], ss_r.at[me], {"sp": k}).wait_send()
            remote(ES.at[k], ER.at[me], es_s.at[k], es_r.at[me], {"sp": k}).wait_send()


def tables(blocks):
    freq = 10000.0 ** (-(np.arange(128) % 32) / 32.0)
    a = np.arange(blocks)[:, None] * 128.0 * freq[None, :]
    r = np.arange(128)[:, None] * freq[None, :]
    return (
        np.stack([np.cos(a), np.sin(a)]).astype(np.float32),
        np.stack([np.cos(r), np.sin(r)]).astype(np.float32),
    )


def local(
    nsp, inputs, mix_gain, w_query, w_key, w_value, query_gain, key_gain, sink_logit, w_inner, w_bmat, w_cmat,
    w_gate, w_step, conv_inner, conv_bmat, conv_cmat, step_bias, decay_rate, decay_offset, start_state,
    group_gain, w_out_attn, w_out_state,
):
    wst = jnp.transpose(w_step, (1, 2, 0)).reshape(16, D)
    off = jnp.transpose(decay_offset, (1, 2, 0)).reshape(16, TOK)
    tabs, rows = tables(nsp * NB)
    hbm = pl.BlockSpec(memory_space=pl.ANY)
    vm = pl.BlockSpec(memory_space=pltpu.VMEM)
    V = pltpu.VMEM
    dma = pltpu.SemaphoreType.DMA
    return pl.pallas_call(
        lambda *refs: kernel(nsp, *refs),
        name="layer",
        out_shape=pltpu.VMEM((TOK // 2, D), bf16),
        in_specs=[hbm] * 25,
        out_specs=vm,
        scratch_shapes=[
            V((512, HALF), bf16), V((512, HALF), bf16), V((512, HALF), bf16), V((512, HALF), bf16),
            V((2, 512, 128), f32),
            V((D, 512), bf16), V((D, 256), bf16), V((D, 512), bf16), V((D, 512), bf16), V((D, 512), bf16),
            V((1024, D), bf16), V((128, D), bf16),
            V((2, NB, 512, 128), bf16), V((2, TOK + 256, 128), bf16), V((2, TOK + 256, 256), bf16),
            V((2, 128, 256), bf16), V((2, 128, 256), bf16),
            V((8, TOK + 16, 128), f32), V((2, 8, 8, 128), f32), V((TOK, 512), f32), V((8, 1024), f32),
            V((TOK, 128), f32), V((TOK, 128), f32),
            V((NB, 16, 128), f32), V((NB, 16, 128), f32), V((TOK, 128), f32),
            V((TOK, 512), bf16), V((TOK, 256), bf16), V((TOK, 256), bf16),
            V((TOK, 1024), f32), V((NB, 8, 1024), f32), V((NB, 128, 1024), f32),
            V((nsp, 16, 512), bf16), V((nsp, 16, 512), bf16), V((8, 128), f32), V((nsp, 8, 128), f32),
            V((nsp, 16, 512), bf16), V((nsp, 16, 512), bf16), V((nsp, 8, 512), f32),
            V((NB, 128, 1024), bf16),
            V((TOK, 512), f32), V((TOK, 1024), bf16), V((512, D), bf16), V((2, 128, 512), f32), V((2, 256, 1024), bf16),
            V((256, 256), bf16), V((2, 512, 128), f32), V((2, 8, 128), f32), V((2, 128, 128), f32),
            V((1, D), f32), V((16, D), bf16), V((1, 64), f32), V((1, 64), f32), pltpu.SMEM((8,), f32),
            V((5, 512), bf16), V((5, 256), bf16), V((5, 256), bf16), pltpu.SMEM((2, 8), f32), pltpu.SMEM((2, 8), f32),
            V((16, TOK), f32), V((1, 512), f32),
            dma((12,)), dma((5,)), dma((14,)), dma((2,)), dma((2,)), dma((2,)), dma((2,)), dma((2,)), dma((2,)),
            dma((nsp,)), dma((nsp,)), dma((nsp,)), dma((nsp,)), dma((nsp,)), dma((nsp,)), dma((4,)), dma((4,)),
        ],
        compiler_params=pltpu.CompilerParams(
            collective_id=0, has_side_effects=True, vmem_limit_bytes=56 * 1024 * 1024
        ),
    )(
        inputs, mix_gain.reshape(1, D), w_query, w_key, w_value, w_inner, w_bmat, w_cmat, w_gate, wst,
        query_gain.reshape(1, 64), key_gain.reshape(1, 64), sink_logit, conv_inner, conv_bmat, conv_cmat,
        step_bias, decay_rate, off, start_state.reshape(2, 512, 128),
        group_gain.reshape(1, 512), w_out_attn, w_out_state, jnp.asarray(tabs), jnp.asarray(rows),
    )


def solution(mesh):
    nsp = mesh.shape["sp"]
    return jax.shard_map(
        lambda *args: local(nsp, *args),
        mesh=mesh,
        in_specs=(
            P(("fs", "sp"), "tp"), P(), P(None, "tp"), P(None, "tp"), P(None, "tp"), P(), P(), P("tp"),
            P(None, "tp"), P(None, "tp"), P(None, "tp"), P(None, "tp"), P(None, None, "tp"),
            P(None, "tp"), P(None, "tp"), P(None, "tp"), P(None, "tp"), P(None, "tp"),
            P("sp", None, "tp"), P("fs", "tp", None, None), P("tp"), P("tp", None), P("tp", None),
        ),
        out_specs=P(("fs", "sp", "tp"), None),
        check_vma=False,
    )
```

```python
import math

import jax
import jax.numpy as jnp
import numpy as np
from jax import lax
from jax.experimental import pallas as pl
from jax.experimental.pallas import tpu as pltpu
from jax.sharding import PartitionSpec as P

D = 2048
HALF = 1024
TOK = 1024
BLK = 128
NB = 8
EPS = 1e-06
LOG2E = math.log2(math.e)
NEG = -1e30
MESH = pl.DeviceIdType.MESH
NT = (((1,), (1,)), ((), ()))
f32 = jnp.float32
bf16 = jnp.bfloat16


def iota(shape, dim):
    return lax.broadcasted_iota(jnp.int32, shape, dim)


def mm(a, b):
    return jnp.dot(a, b, preferred_element_type=f32)


def silu(v):
    h = 0.5 * v
    return h + h * jnp.tanh(h)


def kernel(
    nsp,
    x, gain_, wq, wk, wv, wi, wb, wc, wg, wst_, qgain_, kgain_, sink_, ci_, cb_, cc_,
    bias_, rate_, off_, start, ggain_, woa, wos, tabs, rows,
    out,
    XO0, XO1, XP0, XP1, RS, WQ, WKV, WI, WBC, WG, WO, WST, QM, KD, VD, KVS, KVR, MX, MXR, SG, TAPS,
    COS, SIN, STP, CUM, MT, INN, BA, CA, E1X, FL, BS, SS, SR, FS, FR, ES, ER, EF, ENT,
    WN, AT, PR, SST, SPR, HM, STV, TBV, RWV,
    gain, wst, qgain, kgain, sink, ci, cb, cc, bias, rate, off, ggain,
    asem, lsem, wsem, xs_s, xs_r, hs_s, hs_r, ms_s, ms_r, ss_s, ss_r, fs_s, fs_r, es_s, es_r, ps_s, ps_r,
):
    me = lax.axis_index("sp")
    t = lax.axis_index("tp")
    peer = {"tp": 1 - t}
    left = {"sp": lax.rem(me + nsp - 1, nsp)}
    right = {"sp": lax.rem(me + 1, nsp)}
    XO, XP = (XO0, XO1), (XP0, XP1)

    def remote(src, dst, s, r, dev):
        return pltpu.make_async_remote_copy(
            src_ref=src, dst_ref=dst, send_sem=s, recv_sem=r, device_id=dev, device_id_type=MESH
        )

    barrier = pltpu.get_barrier_semaphore()
    pl.semaphore_signal(barrier, inc=1, device_id=peer, device_id_type=MESH)
    for j in range(1, nsp):
        pl.semaphore_signal(
            barrier, inc=1, device_id={"sp": lax.rem(me + j, nsp)}, device_id_type=MESH
        )

    own = pl.multiple_of(t * HALF, HALF)
    oth = pl.multiple_of((1 - t) * HALF, HALF)
    xl = [pltpu.make_async_copy(x.at[h * 512 : (h + 1) * 512, :], XO[h], lsem.at[h]) for h in range(2)]
    small = [
        pltpu.make_async_copy(start, STV, lsem.at[2]),
        pltpu.make_async_copy(tabs.at[:, pl.ds(pl.multiple_of(me * NB, NB), NB), :], TBV, lsem.at[3]),
        pltpu.make_async_copy(rows, RWV, lsem.at[4]),
    ]
    pieces = [(wk, WKV, 0, 128), (wv, WKV, 128, 128), (wi, WI, 0, 512), (wb, WBC, 0, 256), (wc, WBC, 256, 256)]
    first = [
        pltpu.make_async_copy(w.at[pl.ds(own, HALF), :], d.at[pl.ds(own, HALF), c0 : c0 + n], wsem.at[i])
        for i, (w, d, c0, n) in enumerate(pieces)
    ]
    second = [
        pltpu.make_async_copy(w.at[pl.ds(oth, HALF), :], d.at[pl.ds(oth, HALF), c0 : c0 + n], wsem.at[5 + i])
        for i, (w, d, c0, n) in enumerate(pieces)
    ]
    third = [
        pltpu.make_async_copy(wq, WQ, wsem.at[10]),
        pltpu.make_async_copy(wg, WG, wsem.at[11]),
        pltpu.make_async_copy(woa, WO.at[0:512], wsem.at[12]),
        pltpu.make_async_copy(wos, WO.at[512:1024], wsem.at[13]),
    ]
    args = [
        pltpu.make_async_copy(a, b, asem.at[i])
        for i, (a, b) in enumerate(
            [
                (gain_, gain), (wst_, wst), (qgain_, qgain), (kgain_, kgain), (sink_, sink), (ci_, ci), (cb_, cb),
                (cc_, cc), (bias_, bias), (rate_, rate), (off_, off), (ggain_, ggain),
            ]
        )
    ]
    for c in [args[0], xl[0], args[1]] + first[:2] + args[2:]:
        c.start()

    lane = iota((1, 128), 1)
    lo_half = lane < 64
    first_part = lax.rem(lane, 64) < 32
    g_row, g_col = iota((128, 128), 0), iota((128, 128), 1)
    ones_lanes = jnp.ones((128, 128), bf16)
    HM[...] = jnp.where(iota((256, 256), 0) // 64 == iota((256, 256), 1) // 64, 1.0 / 64, 0.0).astype(bf16)
    WST[...] = jnp.zeros((128, D), bf16)

    def scale(ref, at, h, begin):
        g = gain[0:1, pl.ds(at, HALF)]
        for i in range(8):
            r = i * 64
            v = ref[r : r + 64, :].astype(f32)
            ref[r : r + 64, :] = (v * g).astype(bf16)
            ss = jnp.broadcast_to(jnp.sum(v * v, axis=1, keepdims=True), (64, 128))
            if begin:
                RS[h, r : r + 64, :] = ss
            else:
                RS[h, r : r + 64, :] = lax.rsqrt((RS[h, r : r + 64, :] + ss) * (1.0 / D) + EPS)

    for c in first[2:] + [xl[1]] + small:
        c.start()
    mixed_tiles = [(WI, 0), (WI, 256), (WBC, 0), (WBC, 256)]

    def part_one(h):
        rows_ = slice(h * 512, (h + 1) * 512)
        xs = XO[h][...]
        WN[rows_, 0:256] = mm(xs, WKV[pl.ds(own, HALF), :])
        WN[rows_, 256:384] = lax.dot_general(xs, WST[:, pl.ds(own, HALF)], NT, preferred_element_type=f32)
        if h == 0:
            for c in first[2:]:
                c.wait()
        for n, (w, c0) in enumerate(mixed_tiles):
            E1X[rows_, n * 256 : (n + 1) * 256] = mm(xs, w[pl.ds(own, HALF), c0 : c0 + 256])

    with jax.named_scope("w_xl0"):
        xl[0].wait()
        for c in args[:2]:
            c.wait()
    WST[0:16, :] = wst[...]
    for c in second + third:
        c.start()
    scale(XO[0], own, 0, True)
    with jax.named_scope("w_f0"):
        first[0].wait()
        first[1].wait()
    with jax.named_scope("w_barrier"):
        pl.semaphore_wait(barrier, nsp)
    xc = []
    for h in range(2):
        c = remote(x.at[h * 512 : (h + 1) * 512, :], XP[h], xs_s.at[h], xs_r.at[h], peer)
        c.start()
        xc.append(c)
    part_one(0)
    with jax.named_scope("w_xl1"):
        xl[1].wait()
        for c in small + args[2:]:
            c.wait()
    TAPS[0:5, 0:512] = ci[...].astype(f32)
    TAPS[0:5, 512:768] = cb[...].astype(f32)
    TAPS[0:5, 768:1024] = cc[...].astype(f32)
    qg = jnp.concatenate([qgain[...], qgain[...]], axis=1) * (LOG2E / 8.0)
    kg = jnp.concatenate([kgain[...], kgain[...]], axis=1)
    scale(XO[1], own, 1, True)
    part_one(1)

    for d in range(2):
        for q in range(4):
            SST[d, :, q * 128 : (q + 1) * 128] = STV[d, q * 128 : (q + 1) * 128, :].T
    sign = jnp.where(first_part, -1.0, 1.0).astype(f32)
    for b in range(NB):
        ac, as_ = TBV[0, b : b + 1, :], TBV[1, b : b + 1, :]
        COS[b * BLK : (b + 1) * BLK, :] = ac * RWV[0] - as_ * RWV[1]
        SIN[b * BLK : (b + 1) * BLK, :] = (as_ * RWV[0] + ac * RWV[1]) * sign
    for d in range(2):
        ex_row, ex_col = lax.rem(iota((256, 1024), 0), 128), iota((256, 1024), 1) // 64
        SPR[d] = jnp.where(ex_row == ex_col + 16 * (d + 1), 1.0, 0.0).astype(bf16)

    def rotated(n, r0):
        partner = jnp.where(first_part, pltpu.roll(n, 96, 1), pltpu.roll(n, 32, 1))
        return n * COS[r0 : r0 + 128, :] + partner * SIN[r0 : r0 + 128, :]

    def keep_kv(kb, vb, f0):
        kr, vr = pltpu.roll(kb, 64, 1), pltpu.roll(vb, 64, 1)
        KD[0, f0 : f0 + 128, :] = jnp.where(lo_half, kb, kr).astype(bf16)
        KD[1, f0 : f0 + 128, :] = jnp.where(lo_half, kr, kb).astype(bf16)
        VD[0, f0 : f0 + 128, 0:128] = jnp.where(lo_half, vb, vr).astype(bf16)
        VD[1, f0 : f0 + 128, 0:128] = jnp.where(lo_half, vr, vb).astype(bf16)
        VD[0, f0 : f0 + 128, 128:256] = ones_lanes
        VD[1, f0 : f0 + 128, 128:256] = ones_lanes

    sends = []

    def part_two(h):
        h0 = h * 512
        rows_ = slice(h0, h0 + 512)
        xs = XP[h][...]
        for n, (w, c0) in enumerate(mixed_tiles):
            p = mm(xs, w[pl.ds(oth, HALF), c0 : c0 + 256])
            for q in range(2):
                ct = 2 * n + q
                MX[ct, 8 + h0 : 8 + h0 + 512, :] = (
                    ((p[:, q * 128 : (q + 1) * 128] + E1X[rows_, ct * 128 : (ct + 1) * 128]) * RS[h])
                    .astype(bf16)
                    .astype(f32)
                )
        kv = mm(xs, WKV[pl.ds(oth, HALF), :])
        sp_ = lax.dot_general(xs, WST[:, pl.ds(oth, HALF)], NT, preferred_element_type=f32)
        for i in range(4):
            sub = slice(i * 128, (i + 1) * 128)
            STP[h * 4 + i] = ((sp_[sub] + WN[h0 + i * 128 : h0 + (i + 1) * 128, 256:384]) * RS[h, sub, :]).T[0:16]
        kp = ((kv[:, 0:128] + WN[rows_, 0:128]) * RS[h]).astype(bf16).astype(f32)
        vb = ((kv[:, 128:256] + WN[rows_, 128:256]) * RS[h]).astype(bf16).astype(f32)
        ms = mm((kp * kp).astype(bf16), HM[0:128, 0:128])
        for i in range(4):
            r0 = h0 + i * 128
            sub = slice(i * 128, (i + 1) * 128)
            k = rotated(kp[sub] * lax.rsqrt(ms[sub] + EPS) * kg, r0)
            kb = k.astype(bf16).astype(f32)
            keep_kv(kb, vb[sub], r0 + 128)
            if r0 == 0 or r0 == 896:
                KVS[h, :, 0:128] = kb.astype(bf16)
                KVS[h, :, 128:256] = vb[sub].astype(bf16)
        dev = left if h == 0 else right
        mrow = 8 if h == 0 else TOK
        c = remote(MX.at[:, mrow : mrow + 8, :], MXR.at[1 - h], ms_s.at[h], ms_r.at[1 - h], dev)
        c.start()
        sends.append(c)
        c = remote(KVS.at[h], KVR.at[1 - h], hs_s.at[h], hs_r.at[1 - h], dev)
        c.start()
        sends.append(c)

    row16 = iota((16, 128), 0)
    bias_c = jnp.zeros((16, 128), f32)
    rate_c = jnp.zeros((16, 128), f32)
    for r in range(16):
        bias_c = jnp.where(row16 == r, bias[r // 8, r % 8], bias_c)
        rate_c = jnp.where(row16 == r, rate[r // 8, r % 8], rate_c)
    lane8 = iota((8, 128), 1)

    def steps(b):
        v = STP[b] + bias_c
        step = jnp.maximum(v, 0.0) + jnp.log1p(jnp.exp(-jnp.abs(v)))
        la = (-rate_c * step + off[:, b * BLK : (b + 1) * BLK]) * LOG2E
        cf, cw = la[0:8], la[8:16]
        for k in (1, 2, 4, 8, 16, 32, 64):
            cf = cf + jnp.where(lane8 >= k, pltpu.roll(cf, k, 1), 0.0)
            cw = cw + jnp.where(lane8 < 128 - k, pltpu.roll(cw, 128 - k, 1), 0.0)
        cum = jnp.concatenate([cf, cw], axis=0)
        last = jnp.concatenate([cf[:, 127:128], cw[:, 0:1]], axis=0)
        e1 = jnp.exp2(cum)
        e2 = step * jnp.exp2(last - cum)
        STP[b] = step
        CUM[b] = cum
        MT[b * BLK : (b + 1) * BLK, :] = jnp.concatenate(
            [cum, e1, e2, jnp.zeros((80, 128), f32)], axis=0
        ).T

    def conv(b, ct):
        r0 = b * BLK
        acc = None
        for j in range(5):
            term = MX[ct, r0 + 6 + j : r0 + 6 + j + 128, :] * TAPS[j : j + 1, ct * 128 : (ct + 1) * 128]
            acc = term if acc is None else acc + term
        return silu(acc).astype(bf16)

    def cmat_block(b):
        for ct in (6, 7):
            CA[b * BLK : (b + 1) * BLK, (ct - 6) * 128 : (ct - 5) * 128] = conv(b, ct)

    def pre_block(b):
        r0 = b * BLK
        bts = [None, None]
        for ct in (4, 5, 0, 1, 2, 3):
            act = conv(b, ct)
            if ct >= 4:
                BA[r0 : r0 + 128, (ct - 4) * 128 : (ct - 3) * 128] = act
                bts[ct - 4] = act.astype(f32).T.astype(bf16)
            else:
                INN[r0 : r0 + 128, ct * 128 : (ct + 1) * 128] = act
                if ct % 2 == 0:
                    continue
                g = ct // 2
                for d in range(2):
                    c0 = d * 512 + g * 256
                    loaded = (
                        INN[r0 : r0 + 128, g * 256 : (g + 1) * 256].astype(f32) * BS[b, :, c0 : c0 + 256]
                    ).astype(bf16)
                    BS[b, :, c0 : c0 + 256] = mm(bts[g], loaded)

    def spread(h):
        m = MT[h * 512 : (h + 1) * 512, :]
        hi = m.astype(bf16)
        lo = (m - hi.astype(f32)).astype(bf16)
        both = jnp.concatenate([hi, lo], axis=1)
        for n in range(4):
            c = slice(n * 256, (n + 1) * 256)
            e1x = mm(both, SPR[0, :, c])
            E1X[h * 512 : (h + 1) * 512, c] = e1x
            e2x = mm(both, SPR[1, :, c])
            for i in range(4):
                r = i * 128 + (127 if n < 2 else 0)
                FL[h * 4 + i, 0:1, c] = e1x[r : r + 1, :]
                BS[h * 4 + i, :, c] = e2x[i * 128 : (i + 1) * 128]

    def query(h):
        h0 = h * 512
        p = mm(XO[h][...], WQ[pl.ds(own, HALF), :]) + mm(XP[h][...], WQ[pl.ds(oth, HALF), :])
        qp = [(p[:, q * 128 : (q + 1) * 128] * RS[h]).astype(bf16).astype(f32) for q in range(4)]
        for n in range(2):
            ms = mm(jnp.concatenate([(v * v).astype(bf16) for v in qp[2 * n : 2 * n + 2]], axis=1), HM[...])
            for q in range(2):
                for i in range(4):
                    sub = slice(i * 128, (i + 1) * 128)
                    v = qp[2 * n + q][sub] * lax.rsqrt(ms[sub, q * 128 : (q + 1) * 128] + EPS) * qg
                    v = rotated(v, h0 + i * 128)
                    QM[n, h * 4 + i, q * 256 : q * 256 + 128, :] = jnp.where(lo_half, v, 0.0).astype(bf16)
                    QM[n, h * 4 + i, q * 256 + 128 : q * 256 + 256, :] = jnp.where(lo_half, 0.0, v).astype(bf16)

    def gate_rows(h, i):
        rr = pl.multiple_of(i * 256, 256)
        part = pl.ds(rr, 256)
        p = mm(XO[h][part, :], WG[pl.ds(own, HALF), :]) + mm(XP[h][part, :], WG[pl.ds(oth, HALF), :])
        for q in range(4):
            gp = (p[:, q * 128 : (q + 1) * 128] * RS[h, part, :]).astype(bf16).astype(f32)
            SG[pl.ds(h * 512 + rr, 256), q * 128 : (q + 1) * 128] = silu(gp)

    with jax.named_scope("w_x0"):
        xc[0].wait_recv()
        for c in second:
            c.wait()
    scale(XP[0], oth, 0, False)
    part_two(0)
    with jax.named_scope("w_x1"):
        xc[1].wait_recv()
        third[0].wait()
        third[1].wait()
    scale(XP[1], oth, 1, False)
    part_two(1)
    for b in range(4):
        steps(b)
    spread(0)
    query(0)
    for b in (1, 2):
        pre_block(b)
    for b in range(4, 8):
        steps(b)
    spread(1)
    query(1)
    for b in (3, 4, 5, 6):
        pre_block(b)
    with jax.named_scope("w_halo"):
        for e in range(2):
            remote(MX.at[:, 8:16, :], MXR.at[e], ms_s.at[e], ms_r.at[e], left).wait_recv()
    MX[:, 0:8, :] = jnp.where(me == 0, 0.0, MXR[0])
    MX[:, 8 + TOK : 16 + TOK, :] = jnp.where(me == nsp - 1, 0.0, MXR[1])
    for b in (7, 0):
        pre_block(b)

    fd = FL[0, 0:1, :]
    for b in range(1, NB):
        fd = fd * FL[b, 0:1, :]
    FS[...] = jnp.concatenate([fd[:, i * 128 : (i + 1) * 128] for i in range(8)], axis=0)
    FR[me] = FS[...]

    def chain_out(k):
        n0 = pl.multiple_of(k * 8, 8)
        rf = jnp.zeros((8, 512), f32)
        rb = jnp.zeros((8, 512), f32)
        for b in range(NB):
            rf = FL[b, 0:1, 0:512] * rf + BS[b, pl.ds(n0, 8), 0:512]
            z = NB - 1 - b
            rb = FL[z, 0:1, 512:1024] * rb + BS[z, pl.ds(n0, 8), 512:1024]
        return jnp.concatenate([rf, rb], axis=0).astype(bf16)

    SR[me] = chain_out(me)

    @pl.loop(1, nsp)
    def _(j):
        k = lax.rem(me + j, nsp)
        SS[k] = chain_out(k)
        remote(FS, FR.at[me], fs_s.at[k], fs_r.at[me], {"sp": k}).start()
        remote(SS.at[k], SR.at[me], ss_s.at[k], ss_r.at[me], {"sp": k}).start()

    for b in range(NB):
        cmat_block(b)
    with jax.named_scope("w_kvh"):
        for e in range(2):
            remote(KVS.at[e], KVR.at[e], hs_s.at[e], hs_r.at[e], left).wait_recv()
        for c in sends:
            c.wait_send()
    for e in range(2):
        keep_kv(
            KVR[e, :, 0:128].astype(f32), KVR[e, :, 128:256].astype(f32), 0 if e == 0 else 128 + TOK
        )

    def attend(b, u):
        den = (COS, SIN)[u]
        r0 = pl.multiple_of(b * BLK, BLK)
        off_l = jnp.where((me == 0) & (b == 0), 1024, 0)
        off_r = jnp.where((me == nsp - 1) & (b == NB - 1), 1024, 0)
        keep_l = g_col >= g_row + off_l
        keep_r = g_col <= g_row - off_r
        low, high = [], []
        for z in range(2):
            row, col = iota((64, 128), 0) + z * 64, iota((64, 128), 1)
            low.append(col >= row + off_l)
            high.append(col <= row - off_r)
        for g in range(2):
            s = lax.dot_general(QM[g, b], KD[g, pl.ds(r0, 384), :], NT, preferred_element_type=f32)
            for kt in range(3):
                MX[g * 3 + kt, u * 512 : u * 512 + 512, :] = s[:, kt * 128 : (kt + 1) * 128]
        for g in range(2):
            for j in range(4):
                sk = sink[g * 4 + j] * LOG2E
                for z in range(2):
                    r = j * 128 + z * 64
                    sl = jnp.where(low[z], MX[g * 3, u * 512 + r : u * 512 + r + 64, :], NEG)
                    sm = MX[g * 3 + 1, u * 512 + r : u * 512 + r + 64, :]
                    sr = jnp.where(high[z], MX[g * 3 + 2, u * 512 + r : u * 512 + r + 64, :], NEG)
                    m = jnp.max(jnp.maximum(jnp.maximum(sl, sm), sr), axis=1, keepdims=True)
                    m = jnp.broadcast_to(jnp.maximum(m, sk), (64, 128))
                    WI[u * 1024 + g * 512 + r : u * 1024 + g * 512 + r + 64, 0:128] = jnp.exp2(sl - m).astype(bf16)
                    WI[u * 1024 + g * 512 + r : u * 1024 + g * 512 + r + 64, 128:256] = jnp.exp2(sm - m).astype(bf16)
                    WI[u * 1024 + g * 512 + r : u * 1024 + g * 512 + r + 64, 256:384] = jnp.exp2(sr - m).astype(bf16)
                    den[g * 512 + r : g * 512 + r + 64, :] = jnp.exp2(sk - m)
            o = mm(WI[u * 1024 + g * 512 : u * 1024 + (g + 1) * 512, 0:384], VD[g, pl.ds(r0, 384), :])
            for pair in range(2):
                res = []
                for j in (2 * pair, 2 * pair + 1):
                    sub = slice(j * 128, (j + 1) * 128)
                    res.append(o[sub, 0:128] / (o[sub, 128:256] + den[g * 512 + j * 128 : g * 512 + (j + 1) * 128, :]))
                tile = g * 2 + pair
                AT[pl.ds(r0, 128), tile * 128 : (tile + 1) * 128] = jnp.where(
                    lo_half, res[0], res[1]
                ).astype(bf16)

    def inside(b, u):
        r0 = pl.multiple_of(b * BLK, BLK)
        for g in range(2):
            cm = CA[pl.ds(r0, 128), g * 128 : (g + 1) * 128]
            bm = BA[pl.ds(r0, 128), g * 128 : (g + 1) * 128]
            sc = lax.dot_general(cm, bm, NT, preferred_element_type=f32)
            for pair in range(2):
                tile = g * 2 + pair
                xt = INN[pl.ds(r0, 128), tile * 128 : (tile + 1) * 128].astype(f32)
                for j in range(2):
                    h = tile * 2 + j
                    for z in range(2):
                        row, col = iota((64, 128), 0) + z * 64, iota((64, 128), 1)
                        rz = pl.multiple_of(r0 + z * 64, 64)
                        dif = jnp.where(
                            row >= col,
                            MT[pl.ds(rz, 64), h : h + 1] - CUM[b, h : h + 1, :],
                            MT[pl.ds(rz, 64), 8 + h : 9 + h] - CUM[b, 8 + h : 9 + h, :],
                        )
                        sf, sb = STP[b, h : h + 1, :], STP[b, 8 + h : 9 + h, :]
                        st = jnp.where(row == col, sf + sb, jnp.where(row >= col, sf, sb))
                        WBC[u * 512 + tile * 128 + z * 64 : u * 512 + tile * 128 + z * 64 + 64, j * 128 : (j + 1) * 128] = (
                            sc[z * 64 : z * 64 + 64] * jnp.exp2(dif) * st
                        ).astype(bf16)
                xx = jnp.concatenate(
                    [jnp.where(lo_half, xt, 0.0).astype(bf16), jnp.where(lo_half, 0.0, xt).astype(bf16)],
                    axis=0,
                )
                WN[pl.ds(r0, 128), tile * 128 : (tile + 1) * 128] = mm(WBC[u * 512 + tile * 128 : u * 512 + (tile + 1) * 128, 0:256], xx)

    def two_blocks(h, i):
        b = h * 4 + 2 * i
        gate_rows(h, i)
        for u in range(2):
            attend(b + u, u)
            inside(b + u, u)

    @pl.loop(0, 2)
    def _(i):
        two_blocks(0, i)

    with jax.named_scope("w_s"):
        for j in range(1, nsp):
            k = lax.rem(me + j, nsp)
            remote(FS, FR.at[k], fs_s.at[k], fs_r.at[k], {"sp": k}).wait_recv()
            remote(SS.at[k], SR.at[k], ss_s.at[k], ss_r.at[k], {"sp": k}).wait_recv()

    n0 = pl.multiple_of(me * 8, 8)

    def decay_row(d, which):
        return jnp.concatenate([FR[d, which * 4 + i : which * 4 + i + 1, :] for i in range(4)], axis=1)

    run = SST[0, pl.ds(n0, 8), :]
    for d in range(nsp):
        EF[d] = run
        run = decay_row(d, 0) * run + SR[d].astype(f32)[0:8]
    run = SST[1, pl.ds(n0, 8), :]
    for d in range(nsp - 1, -1, -1):
        ES[d] = jnp.concatenate([EF[d], run], axis=0).astype(bf16)
        run = decay_row(d, 1) * run + SR[d].astype(f32)[8:16]
    ER[me] = ES[me]

    @pl.loop(1, nsp)
    def _(j):
        k = lax.rem(me + j, nsp)
        remote(ES.at[k], ER.at[me], es_s.at[k], es_r.at[me], {"sp": k}).start()

    @pl.loop(0, 2)
    def _(i):
        two_blocks(1, i)

    with jax.named_scope("w_e"):
        for j in range(1, nsp):
            k = lax.rem(me + j, nsp)
            remote(ES.at[k], ER.at[k], es_s.at[k], es_r.at[k], {"sp": k}).wait_recv()

    @pl.loop(0, 8)
    def _(i):
        n1 = pl.multiple_of(i * 16, 16)
        ea = ER[2 * i].astype(f32)
        eb = ER[2 * i + 1].astype(f32)
        rf = jnp.concatenate([ea[0:8], eb[0:8]], axis=0)
        rb = jnp.concatenate([ea[8:16], eb[8:16]], axis=0)
        for b in range(NB):
            ENT[b, pl.ds(n1, 16), 0:512] = rf.astype(bf16)
            rf = FL[b, 0:1, 0:512] * rf + BS[b, pl.ds(n1, 16), 0:512]
            z = NB - 1 - b
            ENT[z, pl.ds(n1, 16), 512:1024] = rb.astype(bf16)
            rb = FL[z, 0:1, 512:1024] * rb + BS[z, pl.ds(n1, 16), 512:1024]

    group_mean = jnp.full((256, 256), 1.0 / 256, bf16)

    def finish(b0):
        for g in range(2):
            c0, c1 = g * 256, (g + 1) * 256
            gated = []
            for i in range(4):
                b = b0 + i
                r0 = pl.multiple_of(b * BLK, BLK)
                cm = CA[pl.ds(r0, 128), g * 128 : (g + 1) * 128]
                tot = (
                    WN[pl.ds(r0, 128), c0:c1]
                    + mm(cm, ENT[b, :, c0:c1]) * E1X[pl.ds(r0, 128), c0:c1]
                    + mm(cm, ENT[b, :, 512 + c0 : 512 + c1]) * E1X[pl.ds(r0, 128), 512 + c0 : 512 + c1]
                )
                gated.append(tot * SG[pl.ds(r0, 128), c0:c1])
            ms = mm(jnp.concatenate([(v * v).astype(bf16) for v in gated], axis=0), group_mean)
            for i in range(4):
                r0 = pl.multiple_of((b0 + i) * BLK, BLK)
                AT[pl.ds(r0, 128), 512 + c0 : 512 + c1] = (
                    gated[i] * lax.rsqrt(ms[i * 128 : (i + 1) * 128] + EPS) * ggain[0:1, c0:c1]
                ).astype(bf16)

    with jax.named_scope("w_wo"):
        third[2].wait()
        third[3].wait()
    other = pl.multiple_of((1 - t) * 512, 512)
    mine = pl.multiple_of(t * 512, 512)
    pc = []

    with jax.named_scope("c_fin0"):
        finish((1 - t) * 4)

    for n in range(4):
        dst = (XO0, XP0)[n // 2].at[:, (n % 2) * 512 : (n % 2) * 512 + 512]
        cols = slice(n * 512, (n + 1) * 512)
        dst[...] = mm(AT[pl.ds(other, 512), :], WO[:, cols]).astype(bf16)
        c = remote(dst, PR.at[:, cols], ps_s.at[n], ps_r.at[n], peer)
        c.start()
        pc.append(c)

    with jax.named_scope("c_fin1"):
        finish(t * 4)

    def own_tile(n):
        dst = (XO1, XP1)[n // 4]
        c0 = (n % 4) * 256
        dst[:, c0 : c0 + 256] = mm(AT[pl.ds(mine, 512), :], WO[:, n * 256 : (n + 1) * 256]).astype(bf16)

    def sum_tile(n):
        own_part = (XO1, XP1)[n // 4][:, (n % 4) * 256 : (n % 4) * 256 + 256].astype(f32)
        out[:, n * 256 : (n + 1) * 256] = (own_part + PR[:, n * 256 : (n + 1) * 256].astype(f32)).astype(bf16)

    with jax.named_scope("c_out1"):
        for n in range(3):
            own_tile(n)
    with jax.named_scope("w_p"):
        for c in pc:
            c.wait_recv()
    with jax.named_scope("c_out2"):
        for n in range(3, 8):
            p = mm(AT[pl.ds(mine, 512), :], WO[:, n * 256 : (n + 1) * 256]).astype(bf16).astype(f32)
            out[:, n * 256 : (n + 1) * 256] = (p + PR[:, n * 256 : (n + 1) * 256].astype(f32)).astype(bf16)
            if n < 6:
                sum_tile(n - 3)

    with jax.named_scope("w_snd"):
        for c in xc + pc:
            c.wait_send()

        @pl.loop(1, nsp)
        def _(j):
            k = lax.rem(me + j, nsp)
            remote(FS, FR.at[me], fs_s.at[k], fs_r.at[me], {"sp": k}).wait_send()
            remote(SS.at[k], SR.at[me], ss_s.at[k], ss_r.at[me], {"sp": k}).wait_send()
            remote(ES.at[k], ER.at[me], es_s.at[k], es_r.at[me], {"sp": k}).wait_send()


def tables(blocks):
    freq = 10000.0 ** (-(np.arange(128) % 32) / 32.0)
    a = np.arange(blocks)[:, None] * 128.0 * freq[None, :]
    r = np.arange(128)[:, None] * freq[None, :]
    return (
        np.stack([np.cos(a), np.sin(a)]).astype(np.float32),
        np.stack([np.cos(r), np.sin(r)]).astype(np.float32),
    )


def local(
    nsp, inputs, mix_gain, w_query, w_key, w_value, query_gain, key_gain, sink_logit, w_inner, w_bmat, w_cmat,
    w_gate, w_step, conv_inner, conv_bmat, conv_cmat, step_bias, decay_rate, decay_offset, start_state,
    group_gain, w_out_attn, w_out_state,
):
    wst = jnp.transpose(w_step, (1, 2, 0)).reshape(16, D)
    off = jnp.transpose(decay_offset, (1, 2, 0)).reshape(16, TOK)
    tabs, rows = tables(nsp * NB)
    hbm = pl.BlockSpec(memory_space=pl.ANY)
    vm = pl.BlockSpec(memory_space=pltpu.VMEM)
    V = pltpu.VMEM
    dma = pltpu.SemaphoreType.DMA
    return pl.pallas_call(
        lambda *refs: kernel(nsp, *refs),
        name="layer",
        out_shape=pltpu.VMEM((TOK // 2, D), bf16),
        in_specs=[hbm] * 25,
        out_specs=vm,
        scratch_shapes=[
            V((512, HALF), bf16), V((512, HALF), bf16), V((512, HALF), bf16), V((512, HALF), bf16),
            V((2, 512, 128), f32),
            V((D, 512), bf16), V((D, 256), bf16), V((D, 512), bf16), V((D, 512), bf16), V((D, 512), bf16),
            V((1024, D), bf16), V((128, D), bf16),
            V((2, NB, 512, 128), bf16), V((2, TOK + 256, 128), bf16), V((2, TOK + 256, 256), bf16),
            V((2, 128, 256), bf16), V((2, 128, 256), bf16),
            V((8, TOK + 16, 128), f32), V((2, 8, 8, 128), f32), V((TOK, 512), f32), V((8, 1024), f32),
            V((TOK, 128), f32), V((TOK, 128), f32),
            V((NB, 16, 128), f32), V((NB, 16, 128), f32), V((TOK, 128), f32),
            V((TOK, 512), bf16), V((TOK, 256), bf16), V((TOK, 256), bf16),
            V((TOK, 1024), f32), V((NB, 8, 1024), f32), V((NB, 128, 1024), f32),
            V((nsp, 16, 512), bf16), V((nsp, 16, 512), bf16), V((8, 128), f32), V((nsp, 8, 128), f32),
            V((nsp, 16, 512), bf16), V((nsp, 16, 512), bf16), V((nsp, 8, 512), f32),
            V((NB, 128, 1024), bf16),
            V((TOK, 512), f32), V((TOK, 1024), bf16), V((512, D), bf16), V((2, 128, 512), f32), V((2, 256, 1024), bf16),
            V((256, 256), bf16), V((2, 512, 128), f32), V((2, 8, 128), f32), V((2, 128, 128), f32),
            V((1, D), f32), V((16, D), bf16), V((1, 64), f32), V((1, 64), f32), pltpu.SMEM((8,), f32),
            V((5, 512), bf16), V((5, 256), bf16), V((5, 256), bf16), pltpu.SMEM((2, 8), f32), pltpu.SMEM((2, 8), f32),
            V((16, TOK), f32), V((1, 512), f32),
            dma((12,)), dma((5,)), dma((14,)), dma((2,)), dma((2,)), dma((2,)), dma((2,)), dma((2,)), dma((2,)),
            dma((nsp,)), dma((nsp,)), dma((nsp,)), dma((nsp,)), dma((nsp,)), dma((nsp,)), dma((4,)), dma((4,)),
        ],
        compiler_params=pltpu.CompilerParams(
            collective_id=0, has_side_effects=True, vmem_limit_bytes=56 * 1024 * 1024
        ),
    )(
        inputs, mix_gain.reshape(1, D), w_query, w_key, w_value, w_inner, w_bmat, w_cmat, w_gate, wst,
        query_gain.reshape(1, 64), key_gain.reshape(1, 64), sink_logit, conv_inner, conv_bmat, conv_cmat,
        step_bias, decay_rate, off, start_state.reshape(2, 512, 128),
        group_gain.reshape(1, 512), w_out_attn, w_out_state, jnp.asarray(tabs), jnp.asarray(rows),
    )


def solution(mesh):
    nsp = mesh.shape["sp"]
    return jax.shard_map(
        lambda *args: local(nsp, *args),
        mesh=mesh,
        in_specs=(
            P(("fs", "sp"), "tp"), P(), P(None, "tp"), P(None, "tp"), P(None, "tp"), P(), P(), P("tp"),
            P(None, "tp"), P(None, "tp"), P(None, "tp"), P(None, "tp"), P(None, None, "tp"),
            P(None, "tp"), P(None, "tp"), P(None, "tp"), P(None, "tp"), P(None, "tp"),
            P("sp", None, "tp"), P("fs", "tp", None, None), P("tp"), P("tp", None), P("tp", None),
        ),
        out_specs=P(("fs", "sp", "tp"), None),
        check_vma=False,
    )
```
